32 devices in a mesh: sp: 8 (over z, y), tp: 4 (over x, core).
Axes of the slice: x: 2, y: 2, z: 4, core: 2. Of those that a mesh axis runs over, the one named last changes fastest.
Arguments:
- residual: bfloat16 [1536, 2048], P(('sp', 'tp')), may hold values from -6 to 6
- mixer_input: bfloat16 [1536, 512], P('sp', 'tp'), may hold values from -6 to 6
- log_gate: float32 [1536, 32], P('sp', 'tp'), may hold values from -2 to 0
- decay_rate: float32 [2, 32, 64], P(None, 'tp'), may hold values from 0 to 1
- turn_rate: float32 [2, 32, 64], P(None, 'tp'), may hold values from -1 to 1
- drive_real: float32 [2, 32, 16, 64], P(None, 'tp'), may hold values from -1 to 1
- drive_imaginary: float32 [2, 32, 16, 64], P(None, 'tp'), may hold values from -1 to 1
- read_real: float32 [2, 32, 16, 64], P(None, 'tp'), may hold values from -0.75 to 0.75
- read_imaginary: float32 [2, 32, 16, 64], P(None, 'tp'), may hold values from -0.75 to 0.75
- skip_gain: float32 [512], P('tp'), may hold values from -4 to 4
- project_weight: bfloat16 [512, 2048], replicated, may hold values from -0.25 to 0.25
- norm_gain: float32 [2048], replicated, may hold values from 0.1 to 1.9
- final_gain: float32 [2048], replicated, may hold values from 0.1 to 1.9
- routes: int32 [1536, 2], P('sp'), may hold values from 0 to 7, all different within a row; in each aligned block of 48 rows (0 to 47, 48 to 95, ...) at most 18 rows name the same one
- group_weight: float32 [1536], P('sp'), may hold values from 0.2 to 1
- expert_weight: float32 [1536, 2], P('sp'), may hold values from 0.1 to 1
- gate_weight: bfloat16 [8, 2048, 1024], P('sp', None, 'tp'), may hold values from -0.125 to 0.125
- linear_weight: bfloat16 [8, 2048, 1024], P('sp', None, 'tp'), may hold values from -0.125 to 0.125
- down_weight: bfloat16 [8, 1024, 2048], P('sp', 'tp'), may hold values from -0.1875 to 0.1875
Outputs:
- finished: bfloat16 [1536, 2048], P(('sp', 'tp'))
The draws below stay inside these ranges and needn't reach their ends.
Inputs may be any that keep to these rules, and one draw needn't show every extreme that they name: `routes`: each row names 2 different experts. In each aligned block of 48 rows no expert is named by more than 18 rows; some expert is named by exactly 18 rows of some block.
All inputs are finite; a program needn't handle non-finite values.
Results may differ from the reference program's by a relative error of at most 0.006.
Values may be sent and summed in bfloat16 or wider, within the bound.
A program may use at most 128 MiB of HBM per device.

```python
import math
import jax
import jax.numpy as jnp
import numpy as np
from jax import lax

D = 2048
S_GROUPS = 32
GROUP_DIM = 16
S_STATE = 64
S_WIDTH = 512
D_EXPERT = 1024
TOP_K = 2
TOK_DEV = 192
TOKENS = 1536
TOK_SHARE = 48
EXPERTS = 8
SLOTS = 18
N_SP = 8
N_TP = 4


def draw_decay_rate(key, part):
    pick_key, fast_key, slow_key = jax.random.split(key, 3)
    fast_share = 0.5
    is_fast = jax.random.uniform(pick_key, (2, S_GROUPS, 1)) < fast_share
    fast_rate = jnp.exp(jax.random.uniform(fast_key, (2, S_GROUPS, S_STATE), minval=jnp.log(0.01), maxval=jnp.log(1.0 / 30.0)))
    slow_rate = jnp.exp(jax.random.uniform(slow_key, (2, S_GROUPS, S_STATE), minval=jnp.log(0.05), maxval=jnp.log(0.3))) / TOKENS
    return jnp.where(is_fast, fast_rate, slow_rate).astype(jnp.float32)


def draw_log_gate(key, part):
    factor_key, rough_key, place_key, drop_key = jax.random.split(key, 4)
    blocks = TOKENS // TOK_DEV
    factor = jnp.exp(jax.random.uniform(factor_key, (blocks, 1, S_GROUPS), minval=0.0, maxval=jnp.log(4.0)))
    roughness = jnp.exp(0.5 * jnp.clip(jax.random.normal(rough_key, (blocks, TOK_DEV, S_GROUPS)), -3.0, 3.0))
    steady = -0.2 / TOKENS * (factor * roughness).reshape(TOKENS, S_GROUPS)
    places = jax.random.randint(place_key, (2,), 0, TOKENS)
    drop_sizes = jnp.log(jax.random.uniform(drop_key, (2, S_GROUPS), minval=0.5, maxval=0.8))
    matches = (jnp.arange(TOKENS, dtype=jnp.int32)[:, None] == places[None, :]).astype(jnp.float32)
    return (steady + jnp.dot(matches, drop_sizes, precision=lax.Precision.HIGHEST)).astype(jnp.float32)


def shard_levels(stream_key, shape, pieces, smallest, high):
    def one(axis_at, shards_of):
        draws = jax.random.uniform(jax.random.fold_in(jax.random.fold_in(stream_key, 6), axis_at), (shards_of,), jnp.float32, smallest / len(pieces), high / len(pieces))
        return jnp.repeat(jnp.exp(draws), shape[axis_at] // shards_of).reshape((-1,) + (1,) * (len(shape) - axis_at - 1))

    level = one(*pieces[0])
    for cut in pieces[1:]:
        level = level * one(*cut)
    return level


def assign_block(rng, own, number, rows, number_of, top, most, skew):
    ranking = jax.random.permutation(rng, number_of)
    heavy_load, common = shares(number_of, rows * top, most, skew, True), shares(number_of, rows * top, most, skew, False)
    places = jnp.arange(number_of)

    def named(tallies, turn):
        used = int((tallies > 0).sum())
        fixed = max(1, used // 4)
        passed = fixed + (places - fixed + turn * (used - fixed)) % max(1, number_of - fixed)
        return jnp.zeros((number_of,), jnp.int32).at[ranking[jnp.where(places < fixed, places, passed)]].set(jnp.asarray(tallies, jnp.int32))

    tallies = jnp.where(number % 4 == 0, named(heavy_load, number // 4), named(common, number - number // 4 - 1))
    mixed = jax.random.permutation(jax.random.fold_in(own, 3), number_of)
    source_of, taker = mixed[0:number_of // 2 * 2:2], mixed[1:number_of // 2 * 2:2]
    room = jnp.minimum(tallies[source_of] - 1, most - tallies[taker]) // 2
    room = jnp.where((source_of == ranking[0]) | (taker == ranking[0]) | (tallies[taker] == 0), 0, jnp.maximum(room, 0))
    passed = jax.random.randint(jax.random.fold_in(own, 4), (number_of // 2,), 0, 1 << 20) % (room + 1)
    tallies = tallies.at[source_of].add(-passed).at[taker].add(passed)
    labels = jnp.searchsorted(jnp.cumsum(tallies), jnp.arange(rows * top), side="right").astype(jnp.int32)
    table = labels.reshape(top, rows).T
    table = table[jax.random.permutation(jax.random.fold_in(own, 1), rows)]
    turn = jax.random.randint(jax.random.fold_in(own, 2), (rows, 1), 0, top)
    return jnp.take_along_axis(table, (jnp.arange(top)[None, :] + turn) % top, axis=1)


def shares(count, total, limit, slope, full):
    weights = [(1 << 20) // math.isqrt(grade ** slope) + 1 for grade in range(1, count + 1)]
    largest = limit if full else min(limit, max(-(-total // count), total * weights[0] // sum(weights)))
    least = 1 if total - largest >= count - 1 else 0
    given, surplus = [largest] + [least] * (count - 1), total - largest - least * (count - 1)
    while surplus > 0:
        candidates = [i for i in range(1, count) if given[i] < largest] or [i for i in range(1, count) if given[i] < limit]
        pool, budget = sum([weights[i] for i in candidates]), surplus
        for i in candidates:
            extra = min(limit - given[i], max(1, budget * weights[i] // pool), surplus)
            given[i] = given[i] + extra
            surplus = surplus - extra
    return np.array(given)


def centred(key, extent, width, most, cuts=(), kind=jnp.bfloat16):
    drawn = width * jax.random.normal(key, extent, jnp.float32)
    if cuts:
        drawn = drawn * shard_levels(key, extent, cuts, -0.22, 0.18)
    return jnp.clip(drawn, -most, most).astype(kind)


def setup_inputs(seed: int = 0) -> dict:
    key_list = jax.random.split(jax.random.key(seed), 20)
    residual = centred(key_list[0], (TOKENS, D), 1.0, 6.0, ((0, 32),))
    mixer_input = centred(key_list[1], (TOKENS, S_WIDTH), 1.0, 6.0, ((0, 8), (1, 4)))
    log_gate = draw_log_gate(jax.random.fold_in(key_list[19], 71), 0)
    decay_rate = draw_decay_rate(jax.random.fold_in(key_list[19], 71), 0)
    turn_rate = jnp.clip(jax.random.uniform(key_list[4], (2, S_GROUPS, S_STATE), jnp.float32, -1.0, 1.0) * shard_levels(key_list[4], (2, S_GROUPS, S_STATE), ((1, 4),), -0.4, 0.0), -1.0, 1.0)
    drive_real = centred(key_list[5], (2, S_GROUPS, GROUP_DIM, S_STATE), (2 * GROUP_DIM) ** -0.5, 1.0, ((1, 4),), jnp.float32)
    drive_imaginary = centred(key_list[6], (2, S_GROUPS, GROUP_DIM, S_STATE), (2 * GROUP_DIM) ** -0.5, 1.0, ((1, 4),), jnp.float32)
    read_real = centred(key_list[7], (2, S_GROUPS, GROUP_DIM, S_STATE), S_STATE ** -0.5, 0.75, ((1, 4),), jnp.float32)
    read_imaginary = centred(key_list[8], (2, S_GROUPS, GROUP_DIM, S_STATE), S_STATE ** -0.5, 0.75, ((1, 4),), jnp.float32)
    skip_gain = centred(key_list[9], (S_WIDTH,), 1.0, 4.0, ((0, 4),), jnp.float32)
    project_weight = centred(key_list[10], (S_WIDTH, D), S_WIDTH ** -0.5, 0.25)
    norm_gain = jnp.clip(1.0 + 0.18 * jax.random.normal(key_list[11], (D,), jnp.float32), 0.1, 1.9)
    final_gain = jnp.clip(1.0 + 0.18 * jax.random.normal(key_list[12], (D,), jnp.float32), 0.1, 1.9)
    routes_keys = jax.random.split(jax.random.fold_in(key_list[13], 1), TOKENS // TOK_SHARE)
    routes_turns = jax.random.permutation(jax.random.fold_in(key_list[13], 3), TOKENS // TOK_SHARE)
    routes = jax.vmap(lambda own, number: assign_block(jax.random.fold_in(key_list[13], 2), own, number, TOK_SHARE, EXPERTS, TOP_K, SLOTS, 2))(routes_keys, routes_turns).reshape((TOKENS, TOP_K))
    group_weight = jnp.clip(jnp.exp(math.log(1.0) - 1.609438 * jax.random.uniform(key_list[14], (TOKENS,), jnp.float32) ** shard_levels(key_list[14], (TOKENS,), ((0, 8),), -0.2, 0.2)), 0.2, 1.0)
    expert_weight = jnp.clip(jnp.exp(math.log(1.0) - 2.3025851 * jax.random.uniform(key_list[15], (TOKENS, TOP_K), jnp.float32) ** shard_levels(key_list[15], (TOKENS, TOP_K), ((0, 8),), -0.2, 0.2)), 0.1, 1.0)
    gate_weight = centred(key_list[16], (EXPERTS, D, D_EXPERT), D ** -0.5, 0.125, ((0, 8), (2, 4)))
    linear_weight = centred(key_list[17], (EXPERTS, D, D_EXPERT), D ** -0.5, 0.125, ((0, 8), (2, 4)))
    down_weight = centred(key_list[18], (EXPERTS, D_EXPERT, D), D_EXPERT ** -0.5, 0.1875, ((0, 8), (1, 4)))
    return {"residual": residual, "mixer_input": mixer_input, "log_gate": log_gate, "decay_rate": decay_rate, "turn_rate": turn_rate, "drive_real": drive_real, "drive_imaginary": drive_imaginary, "read_real": read_real, "read_imaginary": read_imaginary, "skip_gain": skip_gain, "project_weight": project_weight, "norm_gain": norm_gain, "final_gain": final_gain, "routes": routes, "group_weight": group_weight, "expert_weight": expert_weight, "gate_weight": gate_weight, "linear_weight": linear_weight, "down_weight": down_weight}


deep_alpha = 2.0 ** 0.25
norm_epsilon = 1e-05
highest = lax.Precision.HIGHEST

def layer_norm(values, gain):
    center = values - lax.optimization_barrier(jnp.mean(values, axis=-1, keepdims=True))
    spread = lax.optimization_barrier(jnp.mean(center * center, axis=-1, keepdims=True))
    return center * lax.rsqrt(spread + norm_epsilon) * gain

def sweep(inputs, log_gate, rate_row, turn_row, drive_real, drive_imaginary, read_real, read_imaginary, backward):
    input_scale = jnp.sqrt(1.0 - jnp.exp(-2.0 * rate_row))
    retain = jnp.exp(-rate_row)
    step_real = retain * jnp.cos(turn_row)
    step_imaginary = retain * jnp.sin(turn_row)

    def advance(carried, current):
        state_real, state_imaginary = carried
        token_row, gate_row = current
        push_real = jnp.einsum('gh,ghp->gp', token_row, drive_real, precision=highest) * input_scale
        push_imaginary = jnp.einsum('gh,ghp->gp', token_row, drive_imaginary, precision=highest) * input_scale
        factor = jnp.exp(gate_row)[:, None]
        new_real = factor * (step_real * state_real - step_imaginary * state_imaginary) + push_real
        new_imaginary = factor * (step_real * state_imaginary + step_imaginary * state_real) + push_imaginary
        output = jnp.einsum('gp,ghp->gh', new_real, read_real, precision=highest) - jnp.einsum('gp,ghp->gh', new_imaginary, read_imaginary, precision=highest)
        return ((new_real, new_imaginary), output)
    initial = jnp.zeros(rate_row.shape, jnp.float32)
    _, outputs = lax.scan(advance, (initial, initial), (inputs, log_gate), reverse=backward)
    return outputs

def reference(residual, mixer_input, log_gate, decay_rate, turn_rate, drive_real, drive_imaginary, read_real, read_imaginary, skip_gain, project_weight, norm_gain, final_gain, routes, group_weight, expert_weight, gate_weight, linear_weight, down_weight):
    inputs = mixer_input.astype(jnp.float32).reshape(TOKENS, S_GROUPS, GROUP_DIM)
    readout = sweep(inputs, log_gate, decay_rate[0], turn_rate[0], drive_real[0], drive_imaginary[0], read_real[0], read_imaginary[0], False)
    readout = readout + sweep(inputs, log_gate, decay_rate[1], turn_rate[1], drive_real[1], drive_imaginary[1], read_real[1], read_imaginary[1], True)
    readout = readout + skip_gain.reshape(S_GROUPS, GROUP_DIM) * inputs
    activated = jax.nn.gelu(readout).reshape(TOKENS, S_WIDTH).astype(jnp.bfloat16)
    branch = jnp.dot(activated, project_weight, preferred_element_type=jnp.float32)
    middle = layer_norm(deep_alpha * residual.astype(jnp.float32) + branch, norm_gain)
    middle_rows = middle.astype(jnp.bfloat16)
    flat_experts = routes.reshape(-1)
    sorted_order = jnp.argsort(flat_experts, stable=True).astype(jnp.int32)
    counts = lax.optimization_barrier(jnp.sum((flat_experts[:, None] == jnp.arange(EXPERTS, dtype=jnp.int32)[None, :]).astype(jnp.int32), axis=0))
    starts = (jnp.cumsum(counts) - counts).astype(jnp.int32)
    capacity = N_SP * N_TP * SLOTS
    assigned = TOKENS * TOP_K
    piece_width = D_EXPERT // N_TP

    def run_expert(expert):
        offsets = jnp.arange(capacity, dtype=jnp.int32)
        is_valid = offsets < counts[expert]
        chosen = sorted_order[jnp.minimum(starts[expert] + offsets, assigned - 1)]
        row_inputs = middle_rows[chosen // TOP_K]
        gate_part = jnp.dot(row_inputs, gate_weight[expert], preferred_element_type=jnp.float32)
        linear_part = jnp.dot(row_inputs, linear_weight[expert], preferred_element_type=jnp.float32)
        hidden = (jax.nn.silu(gate_part) * linear_part).astype(jnp.bfloat16)
        running = jnp.zeros((capacity, D), jnp.float32)
        for member in range(N_TP):
            partial_value = jnp.dot(hidden[:, member * piece_width:(member + 1) * piece_width], down_weight[expert, member * piece_width:(member + 1) * piece_width], preferred_element_type=jnp.float32)
            rounded = lax.optimization_barrier(partial_value.astype(jnp.bfloat16))
            running = running + rounded.astype(jnp.float32)
        return (running.astype(jnp.bfloat16), jnp.where(is_valid, chosen, assigned).astype(jnp.int32))
    results, targets = lax.map(run_expert, jnp.arange(EXPERTS, dtype=jnp.int32))
    answers = jnp.zeros((assigned, D), jnp.bfloat16).at[targets.reshape(-1)].set(results.reshape(-1, D), mode='drop')
    mixing = group_weight[:, None] * expert_weight / lax.optimization_barrier(jnp.sum(expert_weight, axis=1, keepdims=True))
    routed = lax.optimization_barrier(jnp.sum(mixing[:, :, None] * answers.reshape(TOKENS, TOP_K, D).astype(jnp.float32), axis=1))
    finished = layer_norm(deep_alpha * middle + routed, final_gain)
    return finished.astype(jnp.bfloat16)
```

```python
import functools

import jax
import jax.numpy as jnp
from jax import lax
from jax.experimental import pallas as pl
from jax.experimental.pallas import tpu as pltpu
from jax.sharding import PartitionSpec as P

deep_alpha = 2.0**0.25
norm_epsilon = 1e-05
highest = lax.Precision.HIGHEST
f32 = jnp.float32
bf16 = jnp.bfloat16
segments = 8


def layer_norm(values, gain):
    center = values - jnp.mean(values, axis=-1, keepdims=True)
    spread = jnp.mean(center * center, axis=-1, keepdims=True)
    return center * lax.rsqrt(spread + norm_epsilon) * gain


def iota(shape, axis):
    return lax.broadcasted_iota(jnp.int32, shape, axis)


def exact_dot(a, b, dims=((1,), (0,))):
    return lax.dot_general(a, b, (dims, ((), ())), precision=highest, preferred_element_type=f32)


def mixer_body(n_sp, n_tp, early, linked, sends, refs):
    sources, staged = refs[:12], refs[12:24]
    (push, gate, seg, enter, total, totals, act, chan) = refs[24:32]
    (stage_sems, send_a, recv_a, send_b, recv_b) = refs[32:]
    loads = [
        pltpu.make_async_copy(source, place, stage_sems.at[i])
        for i, (source, place) in enumerate(zip(sources, staged))
    ]
    for load in loads:
        load.start()
    early()
    (x_ref, gate_ref, decay_ref, turn_ref, drive_re, drive_im) = staged[:6]
    (read_re, read_im, skip_ref, residual_ref, gain_ref, weight) = staged[6:]
    sp = lax.axis_index("sp")
    tp = lax.axis_index("tp")
    barrier = pltpu.get_barrier_semaphore()
    for k in range(1, n_sp):
        pl.semaphore_signal(barrier, inc=1, device_id={"sp": lax.rem(sp + k, n_sp)})
    for k in range(1, n_tp):
        pl.semaphore_signal(barrier, inc=1, device_id={"tp": lax.rem(tp + k, n_tp)})
    for load in loads[:6]:
        load.wait()

    length, channels = x_ref.shape
    groups, states = decay_ref.shape[1:]
    width = groups * states
    each = channels // groups
    steps = length // segments
    order = iota((length, length), 0)
    place = iota((length, length), 1)
    shuffle = (place == (order % segments) * steps + order // segments).astype(f32)
    x = jnp.dot(shuffle.astype(bf16), x_ref[...], preferred_element_type=f32)
    spread = (iota((states, width), 1) % states == iota((states, width), 0)).astype(f32)
    own = iota((groups, width), 1) // states == iota((groups, width), 0)
    diagonal = iota((channels, width), 1) // states == iota((channels, width), 0) // each

    def row(values):
        wide = exact_dot(values, spread)
        return jnp.sum(jnp.where(own, wide, 0.0), axis=0, keepdims=True)

    def table(values):
        return jnp.where(diagonal, exact_dot(values, spread), 0.0)

    gates = exact_dot(shuffle, jnp.exp(gate_ref[...]), ((1,), (1,)))
    gate[...] = exact_dot(gates, own.astype(f32))
    turn_rows = []
    for k in range(2):
        rate = decay_ref[k]
        turn = turn_ref[k]
        retain = jnp.exp(-rate)
        scale = row(jnp.sqrt(1.0 - jnp.exp(-2.0 * rate)))
        turn_rows.append((row(retain * jnp.cos(turn)), row(retain * jnp.sin(turn))))
        push[2 * k] = exact_dot(x, table(drive_re[k]) * scale)
        push[2 * k + 1] = exact_dot(x, table(drive_im[k]) * scale)
    (f_re, f_im), (b_re, b_im) = turn_rows

    zero = jnp.zeros((segments, width), f32)
    one = jnp.ones((segments, width), f32)

    def rows_of(j):
        return pl.ds(pl.multiple_of(j * segments, segments), segments)

    def first(j, c):
        out = []
        for k, (sr, si) in enumerate(((f_re, f_im), (b_re, b_im))):
            at = rows_of(j if k == 0 else steps - 1 - j)
            ar, ai, vr, vi = c[4 * k : 4 * k + 4]
            g = gate[at, :]
            mr, mi = g * sr, g * si
            out += [
                mr * ar - mi * ai,
                mr * ai + mi * ar,
                mr * vr - mi * vi + push[2 * k, at, :],
                mr * vi + mi * vr + push[2 * k + 1, at, :],
            ]
        return tuple(out)

    ends = lax.fori_loop(0, steps, first, (one, zero, zero, zero) * 2)
    for i, part in enumerate(ends):
        seg[i] = part

    def link(parts, c):
        ar, ai, vr, vi = parts
        return (ar * c[0] - ai * c[1] + vr, ar * c[1] + ai * c[0] + vi)

    def seg_rows(k, s):
        return [seg[4 * k + i, s : s + 1, :] for i in range(4)]

    for k in range(2):
        span = range(segments) if k == 0 else range(segments - 1, -1, -1)
        decay = (one[:1], zero[:1])
        state = (zero[:1], zero[:1])
        for s in span:
            parts = seg_rows(k, s)
            state = link(parts, state)
            decay = link(parts[:2] + [0.0, 0.0], decay)
        for i, value in enumerate(decay + state):
            total[4 * k + i : 4 * k + i + 1, :] = value
    totals[sp] = total[...]

    pl.semaphore_wait(barrier, n_sp - 1 + n_tp - 1)

    def hand(k):
        peer = lax.rem(sp + k, n_sp)
        return pltpu.make_async_remote_copy(
            src_ref=total,
            dst_ref=totals.at[sp],
            send_sem=send_a.at[k],
            recv_sem=recv_a.at[sp],
            device_id={"sp": peer},
        )

    def arrival(k):
        source = lax.rem(sp + k, n_sp)
        return pltpu.make_async_remote_copy(
            src_ref=total,
            dst_ref=totals.at[source],
            send_sem=send_a.at[k],
            recv_sem=recv_a.at[source],
            device_id={"sp": source},
        )

    for k in range(1, n_sp):
        sends.append(hand(k))
        sends[-1].start()
    linked()
    for load in loads[6:9]:
        load.wait()
    tables = [(table(read_re[k]), table(read_im[k])) for k in range(2)]
    for k in range(1, n_sp):
        arrival(k).wait_recv()

    for k in range(2):
        c = (zero[:1], zero[:1])
        for d in range(n_sp) if k == 0 else range(n_sp - 1, -1, -1):
            new = link([totals[d, 4 * k + i : 4 * k + i + 1, :] for i in range(4)], c)
            counts = d < sp if k == 0 else d > sp
            c = tuple(jnp.where(counts, a, b) for a, b in zip(new, c))
        for s in range(segments) if k == 0 else range(segments - 1, -1, -1):
            enter[2 * k, s : s + 1, :] = c[0]
            enter[2 * k + 1, s : s + 1, :] = c[1]
            c = link(seg_rows(k, s), c)

    def second(j, c):
        out = []
        for k, (sr, si) in enumerate(((f_re, f_im), (b_re, b_im))):
            at = rows_of(j if k == 0 else steps - 1 - j)
            vr, vi = c[2 * k : 2 * k + 2]
            g = gate[at, :]
            mr, mi = g * sr, g * si
            new_re = mr * vr - mi * vi + push[2 * k, at, :]
            new_im = mr * vi + mi * vr + push[2 * k + 1, at, :]
            push[2 * k, at, :] = new_re
            push[2 * k + 1, at, :] = new_im
            out += [new_re, new_im]
        return tuple(out)

    lax.fori_loop(0, steps, second, tuple(enter[i] for i in range(4)))
    over = ((1,), (1,))
    readout = exact_dot(push[0], tables[0][0], over) - exact_dot(push[1], tables[0][1], over)
    readout = readout + (
        exact_dot(push[2], tables[1][0], over) - exact_dot(push[3], tables[1][1], over)
    )
    readout = readout + skip_ref[...] * x
    mixed = jax.nn.gelu(readout).astype(bf16)
    act[...] = lax.dot_general(
        shuffle.astype(bf16), mixed, (((0,), (0,)), ((), ())), preferred_element_type=f32
    ).astype(bf16)

    share = length // n_tp

    def shift(k, out):
        peer = lax.rem(tp + k, n_tp)
        return pltpu.make_async_remote_copy(
            src_ref=act.at[pl.ds(pl.multiple_of(peer * share, share), share)],
            dst_ref=chan.at[tp if out else peer],
            send_sem=send_b.at[k],
            recv_sem=recv_b.at[tp if out else peer],
            device_id={"tp": peer},
        )

    for k in range(1, n_tp):
        sends.append(shift(k, True))
        sends[-1].start()
    chan[tp] = act[pl.ds(pl.multiple_of(tp * share, share), share), :]
    for load in loads[9:]:
        load.wait()
    for k in range(1, n_tp):
        shift(k, False).wait_recv()
    whole = jnp.concatenate([chan[m] for m in range(n_tp)], axis=1)
    branch = jnp.dot(whole, weight[...], preferred_element_type=f32)
    return layer_norm(deep_alpha * residual_ref[...].astype(f32) + branch, gain_ref[...])


def flip(base, k):
    out, bit = base, 1
    while bit <= k:
        if k & bit:
            out = out + bit - 2 * bit * lax.rem(lax.div(base, bit), 2)
        bit *= 2
    return out


def shape_of_block(slots, model):
    while slots % 16 == 0 or 16 % (slots % 16):
        slots += 1
    main, extra = slots // 16, slots % 16
    fold = 16 // extra
    return main, extra, fold, model // fold


def layer_kernel(n_sp, n_tp, slots, *refs):
    mixer_in, refs = refs[:12], refs[12:]
    small_in, refs = refs[:4], refs[4:]
    (gate_hbm, linear_hbm, down_hbm, out_ref), refs = refs[:4], refs[4:]
    mixer_scratch, refs = refs[:25], refs[25:]
    small, refs = refs[:4], refs[4:]
    (middle_ref, rows_out, recv, own, part, got, final, back), refs = refs[:8], refs[8:]
    (gate_w, linear_w, down_w), refs = refs[:3], refs[3:]
    (small_sems, weight_sems, give_sems, take_sems), refs = refs[:4], refs[4:]
    s1, r1, s2, r2, s3, r3, s4, r4 = refs

    sp = lax.axis_index("sp")
    tp = lax.axis_index("tp")
    n_hi = n_tp // 2
    hi = lax.div(tp, 2)
    lo = lax.rem(tp, 2)
    sibling = {"tp": hi * 2 + 1 - lo}
    sends = []

    def remote(src, dst, send, receive, where):
        return pltpu.make_async_remote_copy(
            src_ref=src, dst_ref=dst, send_sem=send, recv_sem=receive, device_id=where
        )

    def go(copy):
        copy.start()
        sends.append(copy)

    width = gate_hbm.shape[2]
    homes = [(gate_hbm, gate_w.at[0]), (linear_hbm, linear_w.at[0]), (down_hbm, down_w.at[0:width])]
    others = [gate_w.at[1], linear_w.at[1], down_w.at[width : 2 * width]]
    fetches = [
        pltpu.make_async_copy(source.at[0], place, weight_sems.at[i])
        for i, (source, place) in enumerate(homes)
    ]
    swaps = [
        remote(homes[i][0].at[0], others[i], give_sems.at[i], take_sems.at[i], sibling)
        for i in range(3)
    ]
    stages = [
        pltpu.make_async_copy(source, place, small_sems.at[i])
        for i, (source, place) in enumerate(zip(small_in, small))
    ]

    def early():
        for copy in stages + fetches:
            copy.start()

    def linked():
        for copy in swaps:
            go(copy)

    middle = mixer_body(n_sp, n_tp, early, linked, sends, mixer_in + mixer_scratch)
    middle_ref[...] = middle
    for copy in stages:
        copy.wait()
    routes_ref, group_ref, shares_ref, gain_ref = small

    share, model = middle.shape
    length = routes_ref.shape[1]
    main, extra, fold, piece = shape_of_block(slots, model)
    per = 16 * main + 16
    line = iota((16, piece), 0) % fold
    masks = [line == c for c in range(fold)]
    keep = [mask.astype(f32).astype(bf16) for mask in masks]

    weights = shares_ref[...]
    weights = group_ref[...] * weights / jnp.sum(weights, axis=0, keepdims=True)
    table = jnp.concatenate([routes_ref[...].astype(f32), weights], axis=0)
    pick = (iota((length, share), 0) == tp * share + iota((length, share), 1)).astype(f32)
    facts = exact_dot(table, pick)
    peers = [flip(sp, k) for k in range(n_sp)]
    expert = lax.bitwise_xor(iota((n_sp, share), 0), jnp.full((n_sp, share), sp, jnp.int32))
    expert = expert.astype(f32)
    first, second = facts[0:1] == expert, facts[1:2] == expert
    uses = jnp.where(first, 1.0, 0.0) + jnp.where(second, 1.0, 0.0)
    amounts = jnp.where(first, facts[2:3], 0.0) + jnp.where(second, facts[3:4], 0.0)
    before = (iota((share, share), 0) < iota((share, share), 1)).astype(bf16)
    rank = jnp.dot(uses.astype(bf16), before, preferred_element_type=f32)
    place = iota((per, share), 0)
    slot = jnp.where(place < 16 * main, place, 16 * main + (place - 16 * main) // fold)
    slot = slot.astype(f32)
    chosen = [
        jnp.where(slot == rank[k : k + 1], uses[k : k + 1], 0.0) for k in range(n_sp)
    ]
    weigh = jnp.concatenate([chosen[k] * amounts[k : k + 1] for k in range(n_sp)], axis=0)
    weigh = weigh.T
    coarse = weigh.astype(bf16)
    fine = (weigh - coarse.astype(f32)).astype(bf16)
    weigh = jnp.concatenate([coarse, fine], axis=0)

    def pack(values, extras, store):
        for i in range(main):
            store(slice(i * model, (i + 1) * model), values[16 * i : 16 * i + 16])
        folded = jnp.where(masks[0], extras[:, :piece], 0.0)
        for c in range(1, fold):
            folded = jnp.where(masks[c], extras[:, c * piece : (c + 1) * piece], folded)
        store(slice(main * model, main * model + piece), folded)

    def unpack(block):
        mains = [block[:, i * model : (i + 1) * model] for i in range(main)]
        tail = block[:, main * model :]
        return mains, jnp.concatenate([tail * keep[c] for c in range(fold)], axis=1)

    rows = jnp.dot(
        jnp.concatenate(chosen, axis=0).astype(bf16),
        middle.astype(bf16),
        preferred_element_type=f32,
    )
    for k in range(n_sp):
        block = rows[k * per : (k + 1) * per]

        def store(columns, values):
            rows_out[k, :, columns] = values.astype(bf16)

        pack(block, block[16 * main :], store)

    def across(j):
        return {"tp": flip(hi, j) * 2 + lo}

    def relay(k):
        if k:
            remote(rows_out.at[k], recv.at[0, k], s1.at[k], r1.at[k], {"sp": peers[k]}).wait_recv()
        source = recv.at[0, k] if k else rows_out.at[0]
        for j in range(1, n_hi):
            go(remote(source, recv.at[j, k], s2.at[j, k], r2.at[j, k], across(j)))

    def compute(ks):
        blocks = [(j, k) for k in ks for j in range(n_hi)]
        mains, extras = [], []
        for j, k in blocks:
            if j:
                remote(
                    recv.at[0, k], recv.at[j, k], s2.at[j, k], r2.at[j, k], across(j)
                ).wait_recv()
            a, b = unpack(recv[j, k] if j or k else rows_out[0])
            mains += a
            extras.append(b)
        x = jnp.concatenate(mains + extras, axis=0)
        count = 16 * len(mains)

        def project(weight):
            value = jnp.concatenate(
                [jnp.dot(x, weight[i], preferred_element_type=f32) for i in range(2)], axis=1
            )
            tail = value[count:].reshape(len(blocks) * extra, fold, 2 * width)
            tail = jnp.sum(tail, axis=1, keepdims=True)
            tail = jnp.broadcast_to(tail, (len(blocks) * extra, fold, 2 * width))
            tail = tail.reshape(len(blocks) * 16, 2 * width)
            return jnp.concatenate([value[:count], tail], axis=0) if count else tail

        hidden = (jax.nn.silu(project(gate_w)) * project(linear_w)).astype(bf16)
        y = jnp.dot(hidden, down_w[...], preferred_element_type=f32)
        for i, (j, k) in enumerate(blocks):

            def store(columns, values):
                if j:
                    part[j, k, :, columns] = values.astype(bf16)
                else:
                    own[k, :, columns] = values

            pack(
                y[16 * main * i : 16 * main * (i + 1)],
                y[count + 16 * i : count + 16 * i + 16],
                store,
            )
            if j:
                go(remote(part.at[j, k], got.at[j, k], s3.at[j, k], r3.at[j, k], across(j)))

    def combine(k):
        value = own[k]
        for j in range(1, n_hi):
            remote(part.at[j, k], got.at[j, k], s3.at[j, k], r3.at[j, k], across(j)).wait_recv()
            value = value + got[j, k].astype(f32)
        if k:
            final[k] = value.astype(bf16)
            go(remote(final.at[k], back.at[k], s4.at[k], r4.at[k], {"sp": peers[k]}))
        else:
            back[0] = value.astype(bf16)

    for k in range(1, n_sp):
        go(remote(rows_out.at[k], recv.at[0, k], s1.at[k], r1.at[k], {"sp": peers[k]}))
    unit = max(1, n_sp // 8)
    rounds = [range(i, i + unit) for i in range(0, n_sp, unit)]
    ahead, behind = 1, 2
    for ks in rounds[:ahead]:
        for k in ks:
            relay(k)
    for fetch in fetches:
        fetch.wait()
    for i in range(len(rounds) + behind):
        for k in rounds[i + ahead] if i + ahead < len(rounds) else ():
            relay(k)
        if i == 0:
            for copy in swaps:
                copy.wait_recv()
        if i < len(rounds):
            compute(rounds[i])
        for k in rounds[i - behind] if i >= behind else ():
            combine(k)

    answers = []
    for k in range(n_sp):
        if k:
            remote(final.at[k], back.at[k], s4.at[k], r4.at[k], {"sp": peers[k]}).wait_recv()
        mains, tail = unpack(back[k])
        answers += mains + [tail]
    routed = jnp.dot(weigh, jnp.concatenate(answers, axis=0), preferred_element_type=f32)
    routed = routed[:share] + routed[share:]
    out_ref[...] = layer_norm(deep_alpha * middle_ref[...] + routed, gain_ref[...]).astype(bf16)
    for copy in sends:
        copy.wait_send()


def on_device(
    residual,
    mixer_input,
    log_gate,
    decay_rate,
    turn_rate,
    drive_real,
    drive_imaginary,
    read_real,
    read_imaginary,
    skip_gain,
    project_weight,
    norm_gain,
    final_gain,
    routes,
    group_weight,
    expert_weight,
    gate_weight,
    linear_weight,
    down_weight,
):
    n_sp = lax.axis_size("sp")
    n_tp = lax.axis_size("tp")
    n_hi = n_tp // 2
    length, channels = mixer_input.shape
    groups, states = decay_rate.shape[1:]
    width = groups * states
    share, model = residual.shape
    hidden = gate_weight.shape[2]
    top = routes.shape[1]
    slots = max(2, 3 * share * top // (2 * n_sp))
    main, extra, fold, piece = shape_of_block(slots, model)
    flat = lambda a: a.reshape(2, channels, states)
    staged = (mixer_input, log_gate.T, decay_rate, turn_rate)
    staged += tuple(flat(a) for a in (drive_real, drive_imaginary, read_real, read_imaginary))
    staged += (skip_gain[None, :], residual, norm_gain[None, :], project_weight)
    small = (routes.T, group_weight[None, :], expert_weight.T, final_gain[None, :])
    operands = staged + small + (gate_weight, linear_weight, down_weight)
    dma = pltpu.SemaphoreType.DMA
    block = (16, main * model + piece)
    return pl.pallas_call(
        functools.partial(layer_kernel, n_sp, n_tp, slots),
        out_shape=jax.ShapeDtypeStruct((share, model), bf16),
        in_specs=[pl.BlockSpec(memory_space=pl.ANY)] * len(operands),
        out_specs=pl.BlockSpec(memory_space=pltpu.VMEM),
        scratch_shapes=[pltpu.VMEM(a.shape, a.dtype) for a in staged]
        + [
            pltpu.VMEM((4, length, width), f32),
            pltpu.VMEM((length, width), f32),
            pltpu.VMEM((8, segments, width), f32),
            pltpu.VMEM((4, segments, width), f32),
            pltpu.VMEM((8, width), f32),
            pltpu.VMEM((n_sp, 8, width), f32),
            pltpu.VMEM((length, channels), bf16),
            pltpu.VMEM((n_tp, share, channels), bf16),
            dma((len(staged),)),
            dma((n_sp,)),
            dma((n_sp,)),
            dma((n_tp,)),
            dma((n_tp,)),
        ]
        + [pltpu.VMEM(a.shape, a.dtype) for a in small]
        + [
            pltpu.VMEM((share, model), f32),
            pltpu.VMEM((n_sp,) + block, bf16),
            pltpu.VMEM((n_hi, n_sp) + block, bf16),
            pltpu.VMEM((n_sp,) + block, f32),
            pltpu.VMEM((n_hi, n_sp) + block, bf16),
            pltpu.VMEM((n_hi, n_sp) + block, bf16),
            pltpu.VMEM((n_sp,) + block, bf16),
            pltpu.VMEM((n_sp,) + block, bf16),
            pltpu.VMEM((2, model, hidden), bf16),
            pltpu.VMEM((2, model, hidden), bf16),
            pltpu.VMEM((2 * hidden, model), bf16),
            dma((len(small),)),
            dma((3,)),
            dma((3,)),
            dma((3,)),
            dma((n_sp,)),
            dma((n_sp,)),
            dma((n_hi, n_sp)),
            dma((n_hi, n_sp)),
            dma((n_hi, n_sp)),
            dma((n_hi, n_sp)),
            dma((n_sp,)),
            dma((n_sp,)),
        ],
        compiler_params=pltpu.CompilerParams(
            collective_id=0, has_side_effects=True, vmem_limit_bytes=60 * 2**20
        ),
        name="layer",
    )(*operands)


def solution(mesh):
    placed = (
        P(("sp", "tp"), None),
        P("sp", "tp"),
        P("sp", "tp"),
        P(None, "tp", None),
        P(None, "tp", None),
        P(None, "tp", None, None),
        P(None, "tp", None, None),
        P(None, "tp", None, None),
        P(None, "tp", None, None),
        P("tp"),
        P(),
        P(),
        P(),
        P("sp", None),
        P("sp"),
        P("sp", None),
        P("sp", None, "tp"),
        P("sp", None, "tp"),
        P("sp", "tp", None),
    )
    return jax.shard_map(
        on_device, mesh=mesh, in_specs=placed, out_specs=P(("sp", "tp"), None), check_vma=False
    )
```

```python
import functools

import jax
import jax.numpy as jnp
from jax import lax
from jax.experimental import pallas as pl
from jax.experimental.pallas import tpu as pltpu
from jax.sharding import PartitionSpec as P

deep_alpha = 2.0**0.25
norm_epsilon = 1e-05
highest = lax.Precision.HIGHEST
f32 = jnp.float32
bf16 = jnp.bfloat16
segments = 8


def layer_norm(values, gain):
    center = values - jnp.mean(values, axis=-1, keepdims=True)
    spread = jnp.mean(center * center, axis=-1, keepdims=True)
    return center * lax.rsqrt(spread + norm_epsilon) * gain


def iota(shape, axis):
    return lax.broadcasted_iota(jnp.int32, shape, axis)


def exact_dot(a, b, dims=((1,), (0,))):
    return lax.dot_general(a, b, (dims, ((), ())), precision=highest, preferred_element_type=f32)


def mixer_body(n_sp, n_tp, early, linked, sends, refs):
    sources, staged = refs[:12], refs[12:24]
    (push, gate, seg, enter, total, totals, act, chan) = refs[24:32]
    (stage_sems, send_a, recv_a, send_b, recv_b) = refs[32:]
    loads = [
        pltpu.make_async_copy(source, place, stage_sems.at[i])
        for i, (source, place) in enumerate(zip(sources, staged))
    ]
    for load in loads:
        load.start()
    early()
    (x_ref, gate_ref, decay_ref, turn_ref, drive_re, drive_im) = staged[:6]
    (read_re, read_im, skip_ref, residual_ref, gain_ref, weight) = staged[6:]
    sp = lax.axis_index("sp")
    tp = lax.axis_index("tp")
    barrier = pltpu.get_barrier_semaphore()
    for k in range(1, n_sp):
        pl.semaphore_signal(barrier, inc=1, device_id={"sp": lax.rem(sp + k, n_sp)})
    for k in range(1, n_tp):
        pl.semaphore_signal(barrier, inc=1, device_id={"tp": lax.rem(tp + k, n_tp)})
    for load in loads[:6]:
        load.wait()

    length, channels = x_ref.shape
    groups, states = decay_ref.shape[1:]
    width = groups * states
    each = channels // groups
    steps = length // segments
    order = iota((length, length), 0)
    place = iota((length, length), 1)
    shuffle = (place == (order % segments) * steps + order // segments).astype(f32)
    x = jnp.dot(shuffle.astype(bf16), x_ref[...], preferred_element_type=f32)
    spread = (iota((states, width), 1) % states == iota((states, width), 0)).astype(f32)
    own = iota((groups, width), 1) // states == iota((groups, width), 0)
    diagonal = iota((channels, width), 1) // states == iota((channels, width), 0) // each

    def row(values):
        wide = exact_dot(values, spread)
        return jnp.sum(jnp.where(own, wide, 0.0), axis=0, keepdims=True)

    def table(values):
        return jnp.where(diagonal, exact_dot(values, spread), 0.0)

    gates = exact_dot(shuffle, jnp.exp(gate_ref[...]), ((1,), (1,)))
    gate[...] = exact_dot(gates, own.astype(f32))
    turn_rows = []
    for k in range(2):
        rate = decay_ref[k]
        turn = turn_ref[k]
        retain = jnp.exp(-rate)
        scale = row(jnp.sqrt(1.0 - jnp.exp(-2.0 * rate)))
        turn_rows.append((row(retain * jnp.cos(turn)), row(retain * jnp.sin(turn))))
        push[2 * k] = exact_dot(x, table(drive_re[k]) * scale)
        push[2 * k + 1] = exact_dot(x, table(drive_im[k]) * scale)
    (f_re, f_im), (b_re, b_im) = turn_rows

    zero = jnp.zeros((segments, width), f32)
    one = jnp.ones((segments, width), f32)

    def rows_of(j):
        return pl.ds(pl.multiple_of(j * segments, segments), segments)

    def first(j, c):
        out = []
        for k, (sr, si) in enumerate(((f_re, f_im), (b_re, b_im))):
            at = rows_of(j if k == 0 else steps - 1 - j)
            ar, ai, vr, vi = c[4 * k : 4 * k + 4]
            g = gate[at, :]
            mr, mi = g * sr, g * si
            out += [
                mr * ar - mi * ai,
                mr * ai + mi * ar,
                mr * vr - mi * vi + push[2 * k, at, :],
                mr * vi + mi * vr + push[2 * k + 1, at, :],
            ]
        return tuple(out)

    ends = lax.fori_loop(0, steps, first, (one, zero, zero, zero) * 2)
    for i, part in enumerate(ends):
        seg[i] = part

    def link(parts, c):
        ar, ai, vr, vi = parts
        return (ar * c[0] - ai * c[1] + vr, ar * c[1] + ai * c[0] + vi)

    def seg_rows(k, s):
        return [seg[4 * k + i, s : s + 1, :] for i in range(4)]

    for k in range(2):
        span = range(segments) if k == 0 else range(segments - 1, -1, -1)
        decay = (one[:1], zero[:1])
        state = (zero[:1], zero[:1])
        for s in span:
            parts = seg_rows(k, s)
            state = link(parts, state)
            decay = link(parts[:2] + [0.0, 0.0], decay)
        for i, value in enumerate(decay + state):
            total[4 * k + i : 4 * k + i + 1, :] = value
    totals[sp] = total[...]

    pl.semaphore_wait(barrier, n_sp - 1 + n_tp - 1)

    def hand(k):
        peer = lax.rem(sp + k, n_sp)
        return pltpu.make_async_remote_copy(
            src_ref=total,
            dst_ref=totals.at[sp],
            send_sem=send_a.at[k],
            recv_sem=recv_a.at[sp],
            device_id={"sp": peer},
        )

    def arrival(k):
        source = lax.rem(sp + k, n_sp)
        return pltpu.make_async_remote_copy(
            src_ref=total,
            dst_ref=totals.at[source],
            send_sem=send_a.at[k],
            recv_sem=recv_a.at[source],
            device_id={"sp": source},
        )

    for k in range(1, n_sp):
        sends.append(hand(k))
        sends[-1].start()
    linked()
    for load in loads[6:9]:
        load.wait()
    tables = [(table(read_re[k]), table(read_im[k])) for k in range(2)]
    for k in range(1, n_sp):
        arrival(k).wait_recv()

    for k in range(2):
        c = (zero[:1], zero[:1])
        for d in range(n_sp) if k == 0 else range(n_sp - 1, -1, -1):
            new = link([totals[d, 4 * k + i : 4 * k + i + 1, :] for i in range(4)], c)
            counts = d < sp if k == 0 else d > sp
            c = tuple(jnp.where(counts, a, b) for a, b in zip(new, c))
        for s in range(segments) if k == 0 else range(segments - 1, -1, -1):
            enter[2 * k, s : s + 1, :] = c[0]
            enter[2 * k + 1, s : s + 1, :] = c[1]
            c = link(seg_rows(k, s), c)

    def second(j, c):
        out = []
        for k, (sr, si) in enumerate(((f_re, f_im), (b_re, b_im))):
            at = rows_of(j if k == 0 else steps - 1 - j)
            vr, vi = c[2 * k : 2 * k + 2]
            g = gate[at, :]
            mr, mi = g * sr, g * si
            new_re = mr * vr - mi * vi + push[2 * k, at, :]
            new_im = mr * vi + mi * vr + push[2 * k + 1, at, :]
            push[2 * k, at, :] = new_re
            push[2 * k + 1, at, :] = new_im
            out += [new_re, new_im]
        return tuple(out)

    lax.fori_loop(0, steps, second, tuple(enter[i] for i in range(4)))
    over = ((1,), (1,))
    readout = exact_dot(push[0], tables[0][0], over) - exact_dot(push[1], tables[0][1], over)
    readout = readout + (
        exact_dot(push[2], tables[1][0], over) - exact_dot(push[3], tables[1][1], over)
    )
    readout = readout + skip_ref[...] * x
    mixed = jax.nn.gelu(readout).astype(bf16)
    act[...] = lax.dot_general(
        shuffle.astype(bf16), mixed, (((0,), (0,)), ((), ())), preferred_element_type=f32
    ).astype(bf16)

    share = length // n_tp

    def shift(k, out):
        peer = lax.rem(tp + k, n_tp)
        return pltpu.make_async_remote_copy(
            src_ref=act.at[pl.ds(pl.multiple_of(peer * share, share), share)],
            dst_ref=chan.at[tp if out else peer],
            send_sem=send_b.at[k],
            recv_sem=recv_b.at[tp if out else peer],
            device_id={"tp": peer},
        )

    for k in range(1, n_tp):
        sends.append(shift(k, True))
        sends[-1].start()
    chan[tp] = act[pl.ds(pl.multiple_of(tp * share, share), share), :]
    for load in loads[9:]:
        load.wait()
    for k in range(1, n_tp):
        shift(k, False).wait_recv()
    whole = jnp.concatenate([chan[m] for m in range(n_tp)], axis=1)
    branch = jnp.dot(whole, weight[...], preferred_element_type=f32)
    return layer_norm(deep_alpha * residual_ref[...].astype(f32) + branch, gain_ref[...])


def flip(base, k):
    out, bit = base, 1
    while bit <= k:
        if k & bit:
            out = out + bit - 2 * bit * lax.rem(lax.div(base, bit), 2)
        bit *= 2
    return out


def shape_of_block(slots, model):
    while slots % 16 == 0 or 16 % (slots % 16):
        slots += 1
    main, extra = slots // 16, slots % 16
    fold = 16 // extra
    return main, extra, fold, model // fold


def layer_kernel(n_sp, n_tp, slots, *refs):
    mixer_in, refs = refs[:12], refs[12:]
    small_in, refs = refs[:4], refs[4:]
    (gate_hbm, linear_hbm, down_hbm, out_ref), refs = refs[:4], refs[4:]
    mixer_scratch, refs = refs[:25], refs[25:]
    small, refs = refs[:4], refs[4:]
    (middle_ref, plain, rows_out, recv, own, part, got, final, back), refs = refs[:9], refs[9:]
    (gate_w, linear_w, down_w), refs = refs[:3], refs[3:]
    (small_sems, weight_sems, give_sems, take_sems), refs = refs[:4], refs[4:]
    s0, r0, s1, r1, s2, r2, s3, r3, s4, r4 = refs

    sp = lax.axis_index("sp")
    tp = lax.axis_index("tp")
    n_hi = n_tp // 2
    hi = lax.div(tp, 2)
    lo = lax.rem(tp, 2)
    sibling = {"tp": hi * 2 + 1 - lo}
    sends = []

    def remote(src, dst, send, receive, where):
        return pltpu.make_async_remote_copy(
            src_ref=src, dst_ref=dst, send_sem=send, recv_sem=receive, device_id=where
        )

    def go(copy):
        copy.start()
        sends.append(copy)

    width = gate_hbm.shape[2]
    homes = [(gate_hbm, gate_w.at[0]), (linear_hbm, linear_w.at[0]), (down_hbm, down_w.at[0:width])]
    others = [gate_w.at[1], linear_w.at[1], down_w.at[width : 2 * width]]
    fetches = [
        pltpu.make_async_copy(source.at[0], place, weight_sems.at[i])
        for i, (source, place) in enumerate(homes)
    ]
    swaps = [
        remote(homes[i][0].at[0], others[i], give_sems.at[i], take_sems.at[i], sibling)
        for i in range(3)
    ]
    stages = [
        pltpu.make_async_copy(source, place, small_sems.at[i])
        for i, (source, place) in enumerate(zip(small_in, small))
    ]

    def early():
        for copy in stages + fetches:
            copy.start()

    def linked():
        for copy in swaps:
            go(copy)

    middle = mixer_body(n_sp, n_tp, early, linked, sends, mixer_in + mixer_scratch)
    middle_ref[...] = middle
    plain[0] = middle.astype(bf16)

    def across(j):
        return {"tp": flip(hi, j) * 2 + lo}

    def crossing(j):
        return remote(plain.at[0], plain.at[j], s0.at[j], r0.at[j], across(j))

    for j in range(1, n_hi):
        go(crossing(j))
    for copy in stages:
        copy.wait()
    routes_ref, group_ref, shares_ref, gain_ref = small

    share, model = middle.shape
    length = routes_ref.shape[1]
    main, extra, fold, piece = shape_of_block(slots, model)
    per = 16 * main + 16
    line = iota((16, piece), 0) % fold
    masks = [line == c for c in range(fold)]
    keep = [mask.astype(f32).astype(bf16) for mask in masks]

    weights = shares_ref[...]
    weights = group_ref[...] * weights / jnp.sum(weights, axis=0, keepdims=True)
    table = jnp.concatenate([routes_ref[...].astype(f32), weights], axis=0)
    def look(member):
        pick = (iota((length, share), 0) == member * share + iota((length, share), 1)).astype(f32)
        return exact_dot(table, pick)

    half = max(1, n_sp // 2)
    upper = lax.div(sp, half)
    depth = sp + upper * (n_sp - 1 - 2 * sp)

    def mirrored(index, side):
        return index + side * (n_sp - 1 - 2 * index)

    peers = [mirrored(flip(depth, k), upper) for k in range(half)]
    peers += [mirrored(k, 1 - upper) for k in range(n_sp - half)]
    mine = [k if k < half else half + depth for k in range(n_sp)]
    expert = jnp.full((n_sp, share), sp, jnp.int32)
    for k in range(1, n_sp):
        expert = jnp.where(iota((n_sp, share), 0) == k, peers[k], expert)
    expert = expert.astype(f32)
    before = (iota((share, share), 0) < iota((share, share), 1)).astype(bf16)
    place = iota((per, share), 0)
    slot = jnp.where(place < 16 * main, place, 16 * main + (place - 16 * main) // fold)
    slot = slot.astype(f32)

    def choose(facts, count):
        first, second = facts[0:1] == expert, facts[1:2] == expert
        uses = jnp.where(first, 1.0, 0.0) + jnp.where(second, 1.0, 0.0)
        amounts = jnp.where(first, facts[2:3], 0.0) + jnp.where(second, facts[3:4], 0.0)
        rank = jnp.dot(uses.astype(bf16), before, preferred_element_type=f32)
        picks = [jnp.where(slot == rank[k : k + 1], uses[k : k + 1], 0.0) for k in range(count)]
        return picks, amounts

    chosen, amounts = choose(look(tp), n_sp)
    theirs = [choose(look(across(j)["tp"]), half)[0] for j in range(1, n_hi)]
    weigh = jnp.concatenate([chosen[k] * amounts[k : k + 1] for k in range(n_sp)], axis=0)
    weigh = weigh.T
    coarse = weigh.astype(bf16)
    fine = (weigh - coarse.astype(f32)).astype(bf16)
    weigh = jnp.concatenate([coarse, fine], axis=0)

    def pack(values, extras, store):
        for i in range(main):
            store(slice(i * model, (i + 1) * model), values[16 * i : 16 * i + 16])
        folded = jnp.where(masks[0], extras[:, :piece], 0.0)
        for c in range(1, fold):
            folded = jnp.where(masks[c], extras[:, c * piece : (c + 1) * piece], folded)
        store(slice(main * model, main * model + piece), folded)

    def unpack(block):
        mains = [block[:, i * model : (i + 1) * model] for i in range(main)]
        tail = block[:, main * model :]
        return mains, jnp.concatenate([tail * keep[c] for c in range(fold)], axis=1)

    def select(picks, j):
        picks = jnp.concatenate(picks, axis=0).astype(bf16)
        rows = jnp.dot(picks, plain[j], preferred_element_type=f32)
        for k in range(picks.shape[0] // per):
            block = rows[k * per : (k + 1) * per]

            def store(columns, values):
                rows_out[j, k, :, columns] = values.astype(bf16)

            pack(block, block[16 * main :], store)

    select(chosen, 0)

    def arrive(k):
        remote(rows_out.at[0, k], recv.at[0, k], s1.at[k], r1.at[k], {"sp": peers[k]}).wait_recv()

    def relay(k):
        arrive(k)
        for j in range(1, n_hi):
            go(remote(recv.at[0, k], recv.at[j, k], s2.at[j, k], r2.at[j, k], across(j)))

    def compute(ks):
        blocks = [(j, k) for k in ks for j in range(n_hi)]
        mains, extras = [], []
        for j, k in blocks:
            if j and k:
                remote(
                    recv.at[0, k], recv.at[j, k], s2.at[j, k], r2.at[j, k], across(j)
                ).wait_recv()
            elif k and k < half:
                arrive(k)
            a, b = unpack(recv[j, k] if k else rows_out[j, 0])
            mains += a
            extras.append(b)
        x = jnp.concatenate(mains + extras, axis=0)
        count = 16 * len(mains)

        def project(weight):
            value = jnp.concatenate(
                [jnp.dot(x, weight[i], preferred_element_type=f32) for i in range(2)], axis=1
            )
            tail = value[count:].reshape(len(blocks) * extra, fold, 2 * width)
            tail = jnp.sum(tail, axis=1, keepdims=True)
            tail = jnp.broadcast_to(tail, (len(blocks) * extra, fold, 2 * width))
            tail = tail.reshape(len(blocks) * 16, 2 * width)
            return jnp.concatenate([value[:count], tail], axis=0) if count else tail

        hidden = (jax.nn.silu(project(gate_w)) * project(linear_w)).astype(bf16)
        y = jnp.dot(hidden, down_w[...], preferred_element_type=f32)
        for i, (j, k) in enumerate(blocks):

            def store(columns, values):
                if j:
                    part[j, k, :, columns] = values.astype(bf16)
                else:
                    own[k, :, columns] = values

            pack(
                y[16 * main * i : 16 * main * (i + 1)],
                y[count + 16 * i : count + 16 * i + 16],
                store,
            )
            if j:
                go(remote(part.at[j, k], got.at[j, k], s3.at[j, k], r3.at[j, k], across(j)))

    def combine(k):
        value = own[k]
        for j in range(1, n_hi):
            remote(part.at[j, k], got.at[j, k], s3.at[j, k], r3.at[j, k], across(j)).wait_recv()
            value = value + got[j, k].astype(f32)
        if k:
            final[k] = value.astype(bf16)
            there = mine[k]
            go(remote(final.at[k], back.at[there], s4.at[k], r4.at[there], {"sp": peers[k]}))
        else:
            back[0] = value.astype(bf16)

    unit = max(1, n_sp // 8)

    def eighth(i):
        return range(i * unit, i * unit + unit)

    for i in (0, 1, 4, 6, 5, 7, 2, 3):
        for k in eighth(i):
            if k:
                there = mine[k]
                go(
                    remote(
                        rows_out.at[0, k],
                        recv.at[0, there],
                        s1.at[k],
                        r1.at[there],
                        {"sp": peers[k]},
                    )
                )
    for j in range(1, n_hi):
        crossing(j).wait_recv()
        select(theirs[j - 1], j)
        for k in range(1, half):
            go(
                remote(
                    rows_out.at[j, k], recv.at[j, k], s2.at[j, k], r2.at[j, k], {"sp": peers[k]}
                )
            )
    for fetch in fetches:
        fetch.wait()
    for copy in swaps:
        copy.wait_recv()
    for step in "r4 c0 r5 c1 c4 b0 r6 c5 b4 b1 c2 r7 c6 b5 b2 c3 c7 b6 b3 b7".split():
        ks = eighth(int(step[1:]))
        if step[0] == "c":
            compute(ks)
        else:
            for k in ks:
                (relay if step[0] == "r" else combine)(k)

    answers = []
    for k in range(n_sp):
        if k:
            remote(final.at[k], back.at[k], s4.at[k], r4.at[k], {"sp": peers[k]}).wait_recv()
        mains, tail = unpack(back[k])
        answers += mains + [tail]
    routed = jnp.dot(weigh, jnp.concatenate(answers, axis=0), preferred_element_type=f32)
    routed = routed[:share] + routed[share:]
    out_ref[...] = layer_norm(deep_alpha * middle_ref[...] + routed, gain_ref[...]).astype(bf16)
    for copy in sends:
        copy.wait_send()


def on_device(
    residual,
    mixer_input,
    log_gate,
    decay_rate,
    turn_rate,
    drive_real,
    drive_imaginary,
    read_real,
    read_imaginary,
    skip_gain,
    project_weight,
    norm_gain,
    final_gain,
    routes,
    group_weight,
    expert_weight,
    gate_weight,
    linear_weight,
    down_weight,
):
    n_sp = lax.axis_size("sp")
    n_tp = lax.axis_size("tp")
    n_hi = n_tp // 2
    length, channels = mixer_input.shape
    groups, states = decay_rate.shape[1:]
    width = groups * states
    share, model = residual.shape
    hidden = gate_weight.shape[2]
    top = routes.shape[1]
    slots = max(2, 3 * share * top // (2 * n_sp))
    main, extra, fold, piece = shape_of_block(slots, model)
    flat = lambda a: a.reshape(2, channels, states)
    staged = (mixer_input, log_gate.T, decay_rate, turn_rate)
    staged += tuple(flat(a) for a in (drive_real, drive_imaginary, read_real, read_imaginary))
    staged += (skip_gain[None, :], residual, norm_gain[None, :], project_weight)
    small = (routes.T, group_weight[None, :], expert_weight.T, final_gain[None, :])
    operands = staged + small + (gate_weight, linear_weight, down_weight)
    dma = pltpu.SemaphoreType.DMA
    block = (16, main * model + piece)
    return pl.pallas_call(
        functools.partial(layer_kernel, n_sp, n_tp, slots),
        out_shape=jax.ShapeDtypeStruct((share, model), bf16),
        in_specs=[pl.BlockSpec(memory_space=pl.ANY)] * len(operands),
        out_specs=pl.BlockSpec(memory_space=pltpu.VMEM),
        scratch_shapes=[pltpu.VMEM(a.shape, a.dtype) for a in staged]
        + [
            pltpu.VMEM((4, length, width), f32),
            pltpu.VMEM((length, width), f32),
            pltpu.VMEM((8, segments, width), f32),
            pltpu.VMEM((4, segments, width), f32),
            pltpu.VMEM((8, width), f32),
            pltpu.VMEM((n_sp, 8, width), f32),
            pltpu.VMEM((length, channels), bf16),
            pltpu.VMEM((n_tp, share, channels), bf16),
            dma((len(staged),)),
            dma((n_sp,)),
            dma((n_sp,)),
            dma((n_tp,)),
            dma((n_tp,)),
        ]
        + [pltpu.VMEM(a.shape, a.dtype) for a in small]
        + [
            pltpu.VMEM((share, model), f32),
            pltpu.VMEM((n_hi, share, model), bf16),
            pltpu.VMEM((n_hi, n_sp) + block, bf16),
            pltpu.VMEM((n_hi, n_sp) + block, bf16),
            pltpu.VMEM((n_sp,) + block, f32),
            pltpu.VMEM((n_hi, n_sp) + block, bf16),
            pltpu.VMEM((n_hi, n_sp) + block, bf16),
            pltpu.VMEM((n_sp,) + block, bf16),
            pltpu.VMEM((n_sp,) + block, bf16),
            pltpu.VMEM((2, model, hidden), bf16),
            pltpu.VMEM((2, model, hidden), bf16),
            pltpu.VMEM((2 * hidden, model), bf16),
            dma((len(small),)),
            dma((3,)),
            dma((3,)),
            dma((3,)),
            dma((n_hi,)),
            dma((n_hi,)),
            dma((n_sp,)),
            dma((n_sp,)),
            dma((n_hi, n_sp)),
            dma((n_hi, n_sp)),
            dma((n_hi, n_sp)),
            dma((n_hi, n_sp)),
            dma((n_sp,)),
            dma((n_sp,)),
        ],
        compiler_params=pltpu.CompilerParams(
            collective_id=0, has_side_effects=True, vmem_limit_bytes=60 * 2**20
        ),
        name="layer",
    )(*operands)


def solution(mesh):
    placed = (
        P(("sp", "tp"), None),
        P("sp", "tp"),
        P("sp", "tp"),
        P(None, "tp", None),
        P(None, "tp", None),
        P(None, "tp", None, None),
        P(None, "tp", None, None),
        P(None, "tp", None, None),
        P(None, "tp", None, None),
        P("tp"),
        P(),
        P(),
        P(),
        P("sp", None),
        P("sp"),
        P("sp", None),
        P("sp", None, "tp"),
        P("sp", None, "tp"),
        P("sp", "tp", None),
    )
    return jax.shard_map(
        on_device, mesh=mesh, in_specs=placed, out_specs=P(("sp", "tp"), None), check_vma=False
    )
```

```python
import functools

import jax
import jax.numpy as jnp
from jax import lax
from jax.experimental import pallas as pl
from jax.experimental.pallas import tpu as pltpu
from jax.sharding import PartitionSpec as P

deep_alpha = 2.0**0.25
norm_epsilon = 1e-05
highest = lax.Precision.HIGHEST
f32 = jnp.float32
bf16 = jnp.bfloat16
segments = 8


def layer_norm(values, gain):
    center = values - jnp.mean(values, axis=-1, keepdims=True)
    spread = jnp.mean(center * center, axis=-1, keepdims=True)
    return center * lax.rsqrt(spread + norm_epsilon) * gain


def iota(shape, axis):
    return lax.broadcasted_iota(jnp.int32, shape, axis)


def exact_dot(a, b, dims=((1,), (0,))):
    return lax.dot_general(a, b, (dims, ((), ())), precision=highest, preferred_element_type=f32)


def pieces(values, count):
    out = []
    for _ in range(count):
        out.append(values.astype(bf16))
        values = values - out[-1].astype(f32)
    return out


def mixer_body(n_sp, n_tp, early, linked, idle, sends, refs):
    sources, staged = refs[:12], refs[12:24]
    (push, gate, seg, enter, total, totals, act, chan) = refs[24:32]
    (stage_sems, send_a, recv_a, send_b, recv_b) = refs[32:]
    loads = [
        pltpu.make_async_copy(source, place, stage_sems.at[i])
        for i, (source, place) in enumerate(zip(sources, staged))
    ]
    for load in loads:
        load.start()
    early()
    (x_ref, gate_ref, decay_ref, turn_ref, drive_re, drive_im) = staged[:6]
    (read_re, read_im, skip_ref, residual_ref, gain_ref, weight) = staged[6:]
    sp = lax.axis_index("sp")
    tp = lax.axis_index("tp")
    barrier = pltpu.get_barrier_semaphore()
    for k in range(1, n_sp):
        pl.semaphore_signal(barrier, inc=1, device_id={"sp": lax.rem(sp + k, n_sp)})
    for k in range(1, n_tp):
        pl.semaphore_signal(barrier, inc=1, device_id={"tp": lax.rem(tp + k, n_tp)})
    for load in loads[:6]:
        load.wait()

    length, channels = x_ref.shape
    groups, states = decay_ref.shape[1:]
    width = groups * states
    each = channels // groups
    steps = length // segments
    order = iota((length, length), 0)
    place = iota((length, length), 1)
    shuffle = (place == (order % segments) * steps + order // segments).astype(f32)
    shuffle = shuffle.astype(bf16)
    x = jnp.dot(shuffle, x_ref[...], preferred_element_type=f32)
    own = iota((groups, width), 1) // states == iota((groups, width), 0)
    diagonal = iota((channels, width), 1) // states == iota((channels, width), 0) // each

    def wide(values):
        return jnp.concatenate([values] * groups, axis=1)

    def row(values):
        return jnp.sum(jnp.where(own, wide(values), 0.0), axis=0, keepdims=True)

    def table(values):
        return jnp.where(diagonal, wide(values), 0.0)

    gates = jnp.concatenate(pieces(jnp.exp(gate_ref[...]), 3), axis=0)
    gates = lax.dot_general(shuffle, gates, (((1,), (1,)), ((), ())), preferred_element_type=f32)
    gate[...] = jnp.dot(
        gates.astype(bf16),
        jnp.concatenate([own.astype(f32).astype(bf16)] * 3, axis=0),
        preferred_element_type=f32,
    )
    twice = x.astype(bf16)
    twice = jnp.concatenate([twice, twice], axis=1)
    turn_rows = []
    for k in range(2):
        rate = decay_ref[k]
        turn = turn_ref[k]
        retain = jnp.exp(-rate)
        scale = row(jnp.sqrt(1.0 - jnp.exp(-2.0 * rate)))
        turn_rows.append((row(retain * jnp.cos(turn)), row(retain * jnp.sin(turn))))
        for i, drive in enumerate((drive_re, drive_im)):
            split = jnp.concatenate(pieces(table(drive[k]) * scale, 2), axis=0)
            push[2 * k + i] = jnp.dot(twice, split, preferred_element_type=f32)
    (f_re, f_im), (b_re, b_im) = turn_rows

    zero = jnp.zeros((segments, width), f32)
    one = jnp.ones((segments, width), f32)

    def rows_of(j):
        return pl.ds(pl.multiple_of(j * segments, segments), segments)

    def first(j, c):
        out = []
        for k, (sr, si) in enumerate(((f_re, f_im), (b_re, b_im))):
            at = rows_of(j if k == 0 else steps - 1 - j)
            kept, vr, vi = c[3 * k : 3 * k + 3]
            g = gate[at, :]
            mr, mi = g * sr, g * si
            out += [
                kept * g,
                mr * vr - mi * vi + push[2 * k, at, :],
                mr * vi + mi * vr + push[2 * k + 1, at, :],
            ]
        return tuple(out)

    def times(a, b):
        return (a[0] * b[0] - a[1] * b[1], a[0] * b[1] + a[1] * b[0])

    def power(base, count):
        if count == 1:
            return base
        root = power(base, count // 2)
        root = times(root, root)
        return times(root, base) if count % 2 else root

    ends = lax.fori_loop(0, steps, first, (one, zero, zero) * 2, unroll=4)
    for k, turned in enumerate(turn_rows):
        kept, vr, vi = ends[3 * k : 3 * k + 3]
        full = power(turned, steps)
        for i, part in enumerate((kept * full[0], kept * full[1], vr, vi)):
            seg[4 * k + i] = part

    def link(parts, c):
        ar, ai, vr, vi = parts
        return (ar * c[0] - ai * c[1] + vr, ar * c[1] + ai * c[0] + vi)

    def seg_rows(k, s):
        return [seg[4 * k + i, s : s + 1, :] for i in range(4)]

    for k in range(2):
        span = range(segments) if k == 0 else range(segments - 1, -1, -1)
        decay = (one[:1], zero[:1])
        state = (zero[:1], zero[:1])
        for s in span:
            parts = seg_rows(k, s)
            state = link(parts, state)
            decay = link(parts[:2] + [0.0, 0.0], decay)
        for i, value in enumerate(decay + state):
            total[4 * k + i : 4 * k + i + 1, :] = value
    totals[sp] = total[...]

    pl.semaphore_wait(barrier, n_sp - 1 + n_tp - 1)

    def hand(k):
        peer = lax.rem(sp + k, n_sp)
        return pltpu.make_async_remote_copy(
            src_ref=total,
            dst_ref=totals.at[sp],
            send_sem=send_a.at[k],
            recv_sem=recv_a.at[sp],
            device_id={"sp": peer},
        )

    def arrival(k):
        source = lax.rem(sp + k, n_sp)
        return pltpu.make_async_remote_copy(
            src_ref=total,
            dst_ref=totals.at[source],
            send_sem=send_a.at[k],
            recv_sem=recv_a.at[source],
            device_id={"sp": source},
        )

    for k in range(1, n_sp):
        sends.append(hand(k))
        sends[-1].start()
    linked()
    for load in loads[6:9]:
        load.wait()
    tables = [value for k in range(2) for value in (table(read_re[k]), -table(read_im[k]))]
    tables = jnp.concatenate(pieces(jnp.concatenate(tables, axis=1), 2), axis=0)
    direct = skip_ref[...] * x
    for k in range(1, n_sp):
        arrival(k).wait_recv()

    for k in range(2):
        c = (zero[:1], zero[:1])
        for d in range(n_sp) if k == 0 else range(n_sp - 1, -1, -1):
            new = link([totals[d, 4 * k + i : 4 * k + i + 1, :] for i in range(4)], c)
            counts = d < sp if k == 0 else d > sp
            c = tuple(jnp.where(counts, a, b) for a, b in zip(new, c))
        for s in range(segments) if k == 0 else range(segments - 1, -1, -1):
            enter[2 * k, s : s + 1, :] = c[0]
            enter[2 * k + 1, s : s + 1, :] = c[1]
            c = link(seg_rows(k, s), c)

    def second(j, c):
        out = []
        for k, (sr, si) in enumerate(((f_re, f_im), (b_re, b_im))):
            at = rows_of(j if k == 0 else steps - 1 - j)
            vr, vi = c[2 * k : 2 * k + 2]
            g = gate[at, :]
            mr, mi = g * sr, g * si
            new_re = mr * vr - mi * vi + push[2 * k, at, :]
            new_im = mr * vi + mi * vr + push[2 * k + 1, at, :]
            push[2 * k, at, :] = new_re
            push[2 * k + 1, at, :] = new_im
            out += [new_re, new_im]
        return tuple(out)

    lax.fori_loop(0, steps, second, tuple(enter[i] for i in range(4)), unroll=4)
    over = (((1,), (1,)), ((), ()))
    readout = direct
    for i in range(4):
        at = slice(i * width, (i + 1) * width)
        coarse, fine = pieces(push[i], 2)
        both = lax.dot_general(coarse, tables[:, at], over, preferred_element_type=f32)
        rest = lax.dot_general(fine, tables[:channels, at], over, preferred_element_type=f32)
        readout = readout + (both[:, :channels] + (both[:, channels:] + rest))
    mixed = jax.nn.gelu(readout).astype(bf16)
    act[...] = lax.dot_general(
        shuffle, mixed, (((0,), (0,)), ((), ())), preferred_element_type=f32
    ).astype(bf16)

    share = length // n_tp

    def shift(k, out):
        peer = lax.rem(tp + k, n_tp)
        return pltpu.make_async_remote_copy(
            src_ref=act.at[pl.ds(pl.multiple_of(peer * share, share), share)],
            dst_ref=chan.at[tp if out else peer],
            send_sem=send_b.at[k],
            recv_sem=recv_b.at[tp if out else peer],
            device_id={"tp": peer},
        )

    for k in range(1, n_tp):
        sends.append(shift(k, True))
        sends[-1].start()
    idle()
    chan[tp] = act[pl.ds(pl.multiple_of(tp * share, share), share), :]
    for load in loads[9:]:
        load.wait()
    for k in range(1, n_tp):
        shift(k, False).wait_recv()
    whole = jnp.concatenate([chan[m] for m in range(n_tp)], axis=1)
    branch = jnp.dot(whole, weight[...], preferred_element_type=f32)
    return layer_norm(deep_alpha * residual_ref[...].astype(f32) + branch, gain_ref[...])


def flip(base, k):
    out, bit = base, 1
    while bit <= k:
        if k & bit:
            out = out + bit - 2 * bit * lax.rem(lax.div(base, bit), 2)
        bit *= 2
    return out


def shape_of_block(slots, model):
    while slots % 16 == 0 or 16 % (slots % 16):
        slots += 1
    main, extra = slots // 16, slots % 16
    fold = 16 // extra
    return main, extra, fold, model // fold


def layer_kernel(n_sp, n_tp, slots, *refs):
    mixer_in, refs = refs[:12], refs[12:]
    small_in, refs = refs[:4], refs[4:]
    (gate_hbm, linear_hbm, down_hbm, out_ref), refs = refs[:4], refs[4:]
    mixer_scratch, refs = refs[:25], refs[25:]
    small, refs = refs[:4], refs[4:]
    (middle_ref, plain, rows_out, recv, own, part, got, final, back), refs = refs[:9], refs[9:]
    (gate_w, linear_w, down_w), refs = refs[:3], refs[3:]
    (small_sems, weight_sems, give_sems, take_sems), refs = refs[:4], refs[4:]
    s0, r0, s1, r1, s2, r2, s3, r3, s4, r4 = refs

    sp = lax.axis_index("sp")
    tp = lax.axis_index("tp")
    n_hi = n_tp // 2
    hi = lax.div(tp, 2)
    lo = lax.rem(tp, 2)
    sibling = {"tp": hi * 2 + 1 - lo}
    sends = []

    def remote(src, dst, send, receive, where):
        return pltpu.make_async_remote_copy(
            src_ref=src, dst_ref=dst, send_sem=send, recv_sem=receive, device_id=where
        )

    def go(copy):
        copy.start()
        sends.append(copy)

    width = gate_hbm.shape[2]
    homes = [(gate_hbm, gate_w.at[0]), (linear_hbm, linear_w.at[0]), (down_hbm, down_w.at[0:width])]
    others = [gate_w.at[1], linear_w.at[1], down_w.at[width : 2 * width]]
    fetches = [
        pltpu.make_async_copy(source.at[0], place, weight_sems.at[i])
        for i, (source, place) in enumerate(homes)
    ]
    swaps = [
        remote(homes[i][0].at[0], others[i], give_sems.at[i], take_sems.at[i], sibling)
        for i in range(3)
    ]
    stages = [
        pltpu.make_async_copy(source, place, small_sems.at[i])
        for i, (source, place) in enumerate(zip(small_in, small))
    ]

    def early():
        for copy in stages + fetches:
            copy.start()

    def linked():
        for copy in swaps:
            go(copy)

    routes_ref, group_ref, shares_ref, gain_ref = small

    share, model = middle_ref.shape
    length = routes_ref.shape[1]
    main, extra, fold, piece = shape_of_block(slots, model)
    per = 16 * main + 16
    line = iota((16, piece), 0) % fold
    masks = [line == c for c in range(fold)]
    keep = [mask.astype(f32).astype(bf16) for mask in masks]

    half = max(1, n_sp // 2)
    upper = lax.div(sp, half)
    depth = sp + upper * (n_sp - 1 - 2 * sp)

    def mirrored(index, side):
        return index + side * (n_sp - 1 - 2 * index)

    peers = [mirrored(flip(depth, k), upper) for k in range(half)]
    peers += [mirrored(k, 1 - upper) for k in range(n_sp - half)]
    mine = [k if k < half else half + depth for k in range(n_sp)]
    prepared = []

    def idle():
        for copy in stages:
            copy.wait()
        prepared.extend(prepare())

    def prepare():
        weights = shares_ref[...]
        weights = group_ref[...] * weights / jnp.sum(weights, axis=0, keepdims=True)
        table = jnp.concatenate([routes_ref[...].astype(f32), weights], axis=0)
        def look(member):
            pick = (iota((length, share), 0) == member * share + iota((length, share), 1)).astype(f32)
            return exact_dot(table, pick)

        expert = jnp.full((n_sp, share), sp, jnp.int32)
        for k in range(1, n_sp):
            expert = jnp.where(iota((n_sp, share), 0) == k, peers[k], expert)
        expert = expert.astype(f32)
        before = (iota((share, share), 0) < iota((share, share), 1)).astype(bf16)
        place = iota((per, share), 0)
        slot = jnp.where(place < 16 * main, place, 16 * main + (place - 16 * main) // fold)
        slot = slot.astype(f32)

        def choose(facts, count):
            first, second = facts[0:1] == expert, facts[1:2] == expert
            uses = jnp.where(first, 1.0, 0.0) + jnp.where(second, 1.0, 0.0)
            amounts = jnp.where(first, facts[2:3], 0.0) + jnp.where(second, facts[3:4], 0.0)
            rank = jnp.dot(uses.astype(bf16), before, preferred_element_type=f32)
            picks = [jnp.where(slot == rank[k : k + 1], uses[k : k + 1], 0.0) for k in range(count)]
            return picks, amounts

        chosen, amounts = choose(look(tp), n_sp)
        theirs = [choose(look(across(j)["tp"]), half)[0] for j in range(1, n_hi)]
        weigh = jnp.concatenate([chosen[k] * amounts[k : k + 1] for k in range(n_sp)], axis=0)
        weigh = weigh.T
        coarse = weigh.astype(bf16)
        fine = (weigh - coarse.astype(f32)).astype(bf16)
        weigh = jnp.concatenate([coarse, fine], axis=0)
        return chosen, theirs, weigh

    def across(j):
        return {"tp": flip(hi, j) * 2 + lo}

    def pack(values, extras, store):
        for i in range(main):
            store(slice(i * model, (i + 1) * model), values[16 * i : 16 * i + 16])
        folded = jnp.where(masks[0], extras[:, :piece], 0.0)
        for c in range(1, fold):
            folded = jnp.where(masks[c], extras[:, c * piece : (c + 1) * piece], folded)
        store(slice(main * model, main * model + piece), folded)

    def unpack(block):
        mains = [block[:, i * model : (i + 1) * model] for i in range(main)]
        tail = block[:, main * model :]
        return mains, jnp.concatenate([tail * keep[c] for c in range(fold)], axis=1)

    def select(picks, j):
        picks = jnp.concatenate(picks, axis=0).astype(bf16)
        rows = jnp.dot(picks, plain[j], preferred_element_type=f32)
        for k in range(picks.shape[0] // per):
            block = rows[k * per : (k + 1) * per]

            def store(columns, values):
                rows_out[j, k, :, columns] = values.astype(bf16)

            pack(block, block[16 * main :], store)

    middle = mixer_body(n_sp, n_tp, early, linked, idle, sends, mixer_in + mixer_scratch)
    middle_ref[...] = middle
    plain[0] = middle.astype(bf16)

    def crossing(j):
        return remote(plain.at[0], plain.at[j], s0.at[j], r0.at[j], across(j))

    for j in range(1, n_hi):
        go(crossing(j))
    chosen, theirs, weigh = prepared
    select(chosen, 0)

    def arrive(k):
        remote(rows_out.at[0, k], recv.at[0, k], s1.at[k], r1.at[k], {"sp": peers[k]}).wait_recv()

    def relay(k):
        arrive(k)
        for j in range(1, n_hi):
            go(remote(recv.at[0, k], recv.at[j, k], s2.at[j, k], r2.at[j, k], across(j)))

    def compute(ks):
        blocks = [(j, k) for k in ks for j in range(n_hi)]
        mains, extras = [], []
        for j, k in blocks:
            if j and k:
                remote(
                    recv.at[0, k], recv.at[j, k], s2.at[j, k], r2.at[j, k], across(j)
                ).wait_recv()
            elif k and k < half:
                arrive(k)
            a, b = unpack(recv[j, k] if k else rows_out[j, 0])
            mains += a
            extras.append(b)
        x = jnp.concatenate(mains + extras, axis=0)
        count = 16 * len(mains)

        def project(weight):
            value = jnp.concatenate(
                [jnp.dot(x, weight[i], preferred_element_type=f32) for i in range(2)], axis=1
            )
            tail = value[count:].reshape(len(blocks) * extra, fold, 2 * width)
            tail = jnp.sum(tail, axis=1, keepdims=True)
            tail = jnp.broadcast_to(tail, (len(blocks) * extra, fold, 2 * width))
            tail = tail.reshape(len(blocks) * 16, 2 * width)
            return jnp.concatenate([value[:count], tail], axis=0) if count else tail

        hidden = (jax.nn.silu(project(gate_w)) * project(linear_w)).astype(bf16)
        y = jnp.dot(hidden, down_w[...], preferred_element_type=f32)
        for i, (j, k) in enumerate(blocks):

            def store(columns, values):
                if j:
                    part[j, k, :, columns] = values.astype(bf16)
                else:
                    own[k, :, columns] = values

            pack(
                y[16 * main * i : 16 * main * (i + 1)],
                y[count + 16 * i : count + 16 * i + 16],
                store,
            )
            if j:
                go(remote(part.at[j, k], got.at[j, k], s3.at[j, k], r3.at[j, k], across(j)))

    def combine(k):
        value = own[k]
        for j in range(1, n_hi):
            remote(part.at[j, k], got.at[j, k], s3.at[j, k], r3.at[j, k], across(j)).wait_recv()
            value = value + got[j, k].astype(f32)
        if k:
            final[k] = value.astype(bf16)
            there = mine[k]
            go(remote(final.at[k], back.at[there], s4.at[k], r4.at[there], {"sp": peers[k]}))
        else:
            back[0] = value.astype(bf16)

    unit = max(1, n_sp // 8)

    def eighth(i):
        return range(i * unit, i * unit + unit)

    for i in (0, 1, 4, 6, 5, 7, 2, 3):
        for k in eighth(i):
            if k:
                there = mine[k]
                go(
                    remote(
                        rows_out.at[0, k],
                        recv.at[0, there],
                        s1.at[k],
                        r1.at[there],
                        {"sp": peers[k]},
                    )
                )
    for j in range(1, n_hi):
        crossing(j).wait_recv()
        select(theirs[j - 1], j)
        for k in range(1, half):
            go(
                remote(
                    rows_out.at[j, k], recv.at[j, k], s2.at[j, k], r2.at[j, k], {"sp": peers[k]}
                )
            )
    for fetch in fetches:
        fetch.wait()
    for copy in swaps:
        copy.wait_recv()
    for step in "r4 c0 r5 c1 c4 b0 r6 c5 b4 b1 c2 r7 c6 b5 b2 c3 c7 b6 b3 b7".split():
        ks = eighth(int(step[1:]))
        if step[0] == "c":
            compute(ks)
        else:
            for k in ks:
                (relay if step[0] == "r" else combine)(k)

    answers = []
    for k in range(n_sp):
        if k:
            remote(final.at[k], back.at[k], s4.at[k], r4.at[k], {"sp": peers[k]}).wait_recv()
        mains, tail = unpack(back[k])
        answers += mains + [tail]
    routed = jnp.dot(weigh, jnp.concatenate(answers, axis=0), preferred_element_type=f32)
    routed = routed[:share] + routed[share:]
    out_ref[...] = layer_norm(deep_alpha * middle_ref[...] + routed, gain_ref[...]).astype(bf16)
    for copy in sends:
        copy.wait_send()


def on_device(
    residual,
    mixer_input,
    log_gate,
    decay_rate,
    turn_rate,
    drive_real,
    drive_imaginary,
    read_real,
    read_imaginary,
    skip_gain,
    project_weight,
    norm_gain,
    final_gain,
    routes,
    group_weight,
    expert_weight,
    gate_weight,
    linear_weight,
    down_weight,
):
    n_sp = lax.axis_size("sp")
    n_tp = lax.axis_size("tp")
    n_hi = n_tp // 2
    length, channels = mixer_input.shape
    groups, states = decay_rate.shape[1:]
    width = groups * states
    share, model = residual.shape
    hidden = gate_weight.shape[2]
    top = routes.shape[1]
    slots = max(2, 3 * share * top // (2 * n_sp))
    main, extra, fold, piece = shape_of_block(slots, model)
    flat = lambda a: a.reshape(2, channels, states)
    staged = (mixer_input, log_gate.T, decay_rate, turn_rate)
    staged += tuple(flat(a) for a in (drive_real, drive_imaginary, read_real, read_imaginary))
    staged += (skip_gain[None, :], residual, norm_gain[None, :], project_weight)
    small = (routes.T, group_weight[None, :], expert_weight.T, final_gain[None, :])
    operands = staged + small + (gate_weight, linear_weight, down_weight)
    dma = pltpu.SemaphoreType.DMA
    block = (16, main * model + piece)
    return pl.pallas_call(
        functools.partial(layer_kernel, n_sp, n_tp, slots),
        out_shape=jax.ShapeDtypeStruct((share, model), bf16),
        in_specs=[pl.BlockSpec(memory_space=pl.ANY)] * len(operands),
        out_specs=pl.BlockSpec(memory_space=pltpu.VMEM),
        scratch_shapes=[pltpu.VMEM(a.shape, a.dtype) for a in staged]
        + [
            pltpu.VMEM((4, length, width), f32),
            pltpu.VMEM((length, width), f32),
            pltpu.VMEM((8, segments, width), f32),
            pltpu.VMEM((4, segments, width), f32),
            pltpu.VMEM((8, width), f32),
            pltpu.VMEM((n_sp, 8, width), f32),
            pltpu.VMEM((length, channels), bf16),
            pltpu.VMEM((n_tp, share, channels), bf16),
            dma((len(staged),)),
            dma((n_sp,)),
            dma((n_sp,)),
            dma((n_tp,)),
            dma((n_tp,)),
        ]
        + [pltpu.VMEM(a.shape, a.dtype) for a in small]
        + [
            pltpu.VMEM((share, model), f32),
            pltpu.VMEM((n_hi, share, model), bf16),
            pltpu.VMEM((n_hi, n_sp) + block, bf16),
            pltpu.VMEM((n_hi, n_sp) + block, bf16),
            pltpu.VMEM((n_sp,) + block, f32),
            pltpu.VMEM((n_hi, n_sp) + block, bf16),
            pltpu.VMEM((n_hi, n_sp) + block, bf16),
            pltpu.VMEM((n_sp,) + block, bf16),
            pltpu.VMEM((n_sp,) + block, bf16),
            pltpu.VMEM((2, model, hidden), bf16),
            pltpu.VMEM((2, model, hidden), bf16),
            pltpu.VMEM((2 * hidden, model), bf16),
            dma((len(small),)),
            dma((3,)),
            dma((3,)),
            dma((3,)),
            dma((n_hi,)),
            dma((n_hi,)),
            dma((n_sp,)),
            dma((n_sp,)),
            dma((n_hi, n_sp)),
            dma((n_hi, n_sp)),
            dma((n_hi, n_sp)),
            dma((n_hi, n_sp)),
            dma((n_sp,)),
            dma((n_sp,)),
        ],
        compiler_params=pltpu.CompilerParams(
            collective_id=0, has_side_effects=True, vmem_limit_bytes=60 * 2**20
        ),
        name="layer",
    )(*operands)


def solution(mesh):
    placed = (
        P(("sp", "tp"), None),
        P("sp", "tp"),
        P("sp", "tp"),
        P(None, "tp", None),
        P(None, "tp", None),
        P(None, "tp", None, None),
        P(None, "tp", None, None),
        P(None, "tp", None, None),
        P(None, "tp", None, None),
        P("tp"),
        P(),
        P(),
        P(),
        P("sp", None),
        P("sp"),
        P("sp", None),
        P("sp", None, "tp"),
        P("sp", None, "tp"),
        P("sp", "tp", None),
    )
    return jax.shard_map(
        on_device, mesh=mesh, in_specs=placed, out_specs=P(("sp", "tp"), None), check_vma=False
    )
```

```python
import functools

import jax
import jax.numpy as jnp
from jax import lax
from jax.experimental import pallas as pl
from jax.experimental.pallas import tpu as pltpu
from jax.sharding import PartitionSpec as P

deep_alpha = 2.0**0.25
norm_epsilon = 1e-05
highest = lax.Precision.HIGHEST
f32 = jnp.float32
bf16 = jnp.bfloat16
segments = 8


def layer_norm(values, gain):
    center = values - jnp.mean(values, axis=-1, keepdims=True)
    spread = jnp.mean(center * center, axis=-1, keepdims=True)
    return center * lax.rsqrt(spread + norm_epsilon) * gain


def iota(shape, axis):
    return lax.broadcasted_iota(jnp.int32, shape, axis)


def exact_dot(a, b, dims=((1,), (0,))):
    return lax.dot_general(a, b, (dims, ((), ())), precision=highest, preferred_element_type=f32)


def pieces(values, count):
    out = []
    for _ in range(count):
        out.append(values.astype(bf16))
        values = values - out[-1].astype(f32)
    return out


def mixer_body(n_sp, n_tp, early, linked, idle, sends, refs):
    sources, staged = refs[:12], refs[12:24]
    (push, gate, seg, enter, total, totals, act, chan) = refs[24:32]
    (stage_sems, send_a, recv_a, send_b, recv_b) = refs[32:]
    loads = [
        pltpu.make_async_copy(source, place, stage_sems.at[i])
        for i, (source, place) in enumerate(zip(sources, staged))
    ]
    for load in loads:
        load.start()
    early()
    (x_ref, gate_ref, decay_ref, turn_ref, drive_re, drive_im) = staged[:6]
    (read_re, read_im, skip_ref, residual_ref, gain_ref, weight) = staged[6:]
    sp = lax.axis_index("sp")
    tp = lax.axis_index("tp")
    barrier = pltpu.get_barrier_semaphore()
    for k in range(1, n_sp):
        pl.semaphore_signal(barrier, inc=1, device_id={"sp": lax.rem(sp + k, n_sp)})
    for k in range(1, n_tp):
        pl.semaphore_signal(barrier, inc=1, device_id={"tp": lax.rem(tp + k, n_tp)})
    for load in loads[:6]:
        load.wait()

    length, channels = x_ref.shape
    groups, states = decay_ref.shape[1:]
    width = groups * states
    each = channels // groups
    steps = length // segments
    order = iota((length, length), 0)
    place = iota((length, length), 1)
    shuffle = (place == (order % segments) * steps + order // segments).astype(f32)
    shuffle = shuffle.astype(bf16)
    x = jnp.dot(shuffle, x_ref[...], preferred_element_type=f32)
    own = iota((groups, width), 1) // states == iota((groups, width), 0)
    diagonal = iota((channels, width), 1) // states == iota((channels, width), 0) // each

    def wide(values):
        return jnp.concatenate([values] * groups, axis=1)

    def row(values):
        return jnp.sum(jnp.where(own, wide(values), 0.0), axis=0, keepdims=True)

    def table(values):
        return jnp.where(diagonal, wide(values), 0.0)

    gates = jnp.concatenate(pieces(jnp.exp(gate_ref[...]), 3), axis=0)
    gates = lax.dot_general(shuffle, gates, (((1,), (1,)), ((), ())), preferred_element_type=f32)
    gate[...] = jnp.dot(
        gates.astype(bf16),
        jnp.concatenate([own.astype(f32).astype(bf16)] * 3, axis=0),
        preferred_element_type=f32,
    )
    twice = x.astype(bf16)
    twice = jnp.concatenate([twice, twice], axis=1)
    turn_rows = []
    for k in range(2):
        rate = decay_ref[k]
        turn = turn_ref[k]
        retain = jnp.exp(-rate)
        scale = row(jnp.sqrt(1.0 - jnp.exp(-2.0 * rate)))
        turn_rows.append((row(retain * jnp.cos(turn)), row(retain * jnp.sin(turn))))
        for i, drive in enumerate((drive_re, drive_im)):
            split = jnp.concatenate(pieces(table(drive[k]) * scale, 2), axis=0)
            push[2 * k + i] = jnp.dot(twice, split, preferred_element_type=f32)
    (f_re, f_im), (b_re, b_im) = turn_rows

    zero = jnp.zeros((segments, width), f32)
    one = jnp.ones((segments, width), f32)

    def rows_of(j):
        return pl.ds(pl.multiple_of(j * segments, segments), segments)

    def first(j, c):
        out = []
        for k, (sr, si) in enumerate(((f_re, f_im), (b_re, b_im))):
            at = rows_of(j if k == 0 else steps - 1 - j)
            kept, vr, vi = c[3 * k : 3 * k + 3]
            g = gate[at, :]
            mr, mi = g * sr, g * si
            out += [
                kept * g,
                mr * vr - mi * vi + push[2 * k, at, :],
                mr * vi + mi * vr + push[2 * k + 1, at, :],
            ]
        return tuple(out)

    def times(a, b):
        return (a[0] * b[0] - a[1] * b[1], a[0] * b[1] + a[1] * b[0])

    def power(base, count):
        if count == 1:
            return base
        root = power(base, count // 2)
        root = times(root, root)
        return times(root, base) if count % 2 else root

    ends = lax.fori_loop(0, steps, first, (one, zero, zero) * 2, unroll=4)
    for k, turned in enumerate(turn_rows):
        kept, vr, vi = ends[3 * k : 3 * k + 3]
        full = power(turned, steps)
        for i, part in enumerate((kept * full[0], kept * full[1], vr, vi)):
            seg[4 * k + i] = part

    def link(parts, c):
        ar, ai, vr, vi = parts
        return (ar * c[0] - ai * c[1] + vr, ar * c[1] + ai * c[0] + vi)

    def seg_rows(k, s):
        return [seg[4 * k + i, s : s + 1, :] for i in range(4)]

    for k in range(2):
        span = range(segments) if k == 0 else range(segments - 1, -1, -1)
        decay = (one[:1], zero[:1])
        state = (zero[:1], zero[:1])
        for s in span:
            parts = seg_rows(k, s)
            state = link(parts, state)
            decay = link(parts[:2] + [0.0, 0.0], decay)
        for i, value in enumerate(decay + state):
            total[4 * k + i : 4 * k + i + 1, :] = value
    totals[sp] = total[...]

    pl.semaphore_wait(barrier, n_sp - 1 + n_tp - 1)

    def hand(k):
        peer = lax.rem(sp + k, n_sp)
        return pltpu.make_async_remote_copy(
            src_ref=total,
            dst_ref=totals.at[sp],
            send_sem=send_a.at[k],
            recv_sem=recv_a.at[sp],
            device_id={"sp": peer},
        )

    def arrival(k):
        source = lax.rem(sp + k, n_sp)
        return pltpu.make_async_remote_copy(
            src_ref=total,
            dst_ref=totals.at[source],
            send_sem=send_a.at[k],
            recv_sem=recv_a.at[source],
            device_id={"sp": source},
        )

    for k in range(1, n_sp):
        sends.append(hand(k))
        sends[-1].start()
    for load in loads[6:9]:
        load.wait()
    tables = [value for k in range(2) for value in (table(read_re[k]), -table(read_im[k]))]
    tables = jnp.concatenate(pieces(jnp.concatenate(tables, axis=1), 2), axis=0)
    direct = skip_ref[...] * x
    for k in range(1, n_sp):
        arrival(k).wait_recv()

    linked()
    for k in range(2):
        c = (zero[:1], zero[:1])
        for d in range(n_sp) if k == 0 else range(n_sp - 1, -1, -1):
            new = link([totals[d, 4 * k + i : 4 * k + i + 1, :] for i in range(4)], c)
            counts = d < sp if k == 0 else d > sp
            c = tuple(jnp.where(counts, a, b) for a, b in zip(new, c))
        for s in range(segments) if k == 0 else range(segments - 1, -1, -1):
            enter[2 * k, s : s + 1, :] = c[0]
            enter[2 * k + 1, s : s + 1, :] = c[1]
            c = link(seg_rows(k, s), c)

    def second(j, c):
        out = []
        for k, (sr, si) in enumerate(((f_re, f_im), (b_re, b_im))):
            at = rows_of(j if k == 0 else steps - 1 - j)
            vr, vi = c[2 * k : 2 * k + 2]
            g = gate[at, :]
            mr, mi = g * sr, g * si
            new_re = mr * vr - mi * vi + push[2 * k, at, :]
            new_im = mr * vi + mi * vr + push[2 * k + 1, at, :]
            push[2 * k, at, :] = new_re
            push[2 * k + 1, at, :] = new_im
            out += [new_re, new_im]
        return tuple(out)

    lax.fori_loop(0, steps, second, tuple(enter[i] for i in range(4)), unroll=4)
    over = (((1,), (1,)), ((), ()))
    readout = direct
    for i in range(4):
        at = slice(i * width, (i + 1) * width)
        coarse, fine = pieces(push[i], 2)
        both = lax.dot_general(coarse, tables[:, at], over, preferred_element_type=f32)
        rest = lax.dot_general(fine, tables[:channels, at], over, preferred_element_type=f32)
        readout = readout + (both[:, :channels] + (both[:, channels:] + rest))
    mixed = jax.nn.gelu(readout).astype(bf16)
    act[...] = lax.dot_general(
        shuffle, mixed, (((0,), (0,)), ((), ())), preferred_element_type=f32
    ).astype(bf16)

    share = length // n_tp

    def shift(k, out):
        peer = lax.rem(tp + k, n_tp)
        return pltpu.make_async_remote_copy(
            src_ref=act.at[pl.ds(pl.multiple_of(peer * share, share), share)],
            dst_ref=chan.at[tp if out else peer],
            send_sem=send_b.at[k],
            recv_sem=recv_b.at[tp if out else peer],
            device_id={"tp": peer},
        )

    for k in range(1, n_tp):
        sends.append(shift(k, True))
        sends[-1].start()
    idle()
    chan[tp] = act[pl.ds(pl.multiple_of(tp * share, share), share), :]
    for load in loads[9:]:
        load.wait()
    for k in range(1, n_tp):
        shift(k, False).wait_recv()
    whole = jnp.concatenate([chan[m] for m in range(n_tp)], axis=1)
    branch = jnp.dot(whole, weight[...], preferred_element_type=f32)
    return layer_norm(deep_alpha * residual_ref[...].astype(f32) + branch, gain_ref[...])


def flip(base, k):
    out, bit = base, 1
    while bit <= k:
        if k & bit:
            out = out + bit - 2 * bit * lax.rem(lax.div(base, bit), 2)
        bit *= 2
    return out


def shape_of_block(slots, model):
    while slots % 16 == 0 or 16 % (slots % 16):
        slots += 1
    main, extra = slots // 16, slots % 16
    fold = 16 // extra
    return main, extra, fold, model // fold


def layer_kernel(n_sp, n_tp, slots, *refs):
    mixer_in, refs = refs[:12], refs[12:]
    small_in, refs = refs[:4], refs[4:]
    (gate_hbm, linear_hbm, down_hbm, out_ref), refs = refs[:4], refs[4:]
    mixer_scratch, refs = refs[:25], refs[25:]
    small, refs = refs[:4], refs[4:]
    (middle_ref, plain, rows_out, recv, own, part, got, final, back), refs = refs[:9], refs[9:]
    (gate_w, linear_w, down_w), refs = refs[:3], refs[3:]
    (small_sems, weight_sems, give_sems, take_sems), refs = refs[:4], refs[4:]
    s0, r0, s1, r1, s2, r2, s3, r3, s4, r4 = refs

    sp = lax.axis_index("sp")
    tp = lax.axis_index("tp")
    n_hi = n_tp // 2
    hi = lax.div(tp, 2)
    lo = lax.rem(tp, 2)
    sibling = {"tp": hi * 2 + 1 - lo}
    sends = []

    def remote(src, dst, send, receive, where):
        return pltpu.make_async_remote_copy(
            src_ref=src, dst_ref=dst, send_sem=send, recv_sem=receive, device_id=where
        )

    def go(copy):
        copy.start()
        sends.append(copy)

    width = gate_hbm.shape[2]
    homes = [(gate_hbm, gate_w.at[0]), (linear_hbm, linear_w.at[0]), (down_hbm, down_w.at[0:width])]
    others = [gate_w.at[1], linear_w.at[1], down_w.at[width : 2 * width]]
    fetches = [
        pltpu.make_async_copy(source.at[0], place, weight_sems.at[i])
        for i, (source, place) in enumerate(homes)
    ]
    swaps = [
        remote(homes[i][0].at[0], others[i], give_sems.at[i], take_sems.at[i], sibling)
        for i in range(3)
    ]
    stages = [
        pltpu.make_async_copy(source, place, small_sems.at[i])
        for i, (source, place) in enumerate(zip(small_in, small))
    ]

    def early():
        for copy in stages + fetches:
            copy.start()

    def linked():
        for copy in swaps:
            go(copy)

    routes_ref, group_ref, shares_ref, gain_ref = small

    share, model = middle_ref.shape
    length = routes_ref.shape[1]
    main, extra, fold, piece = shape_of_block(slots, model)
    per = 16 * main + 16
    line = iota((16, piece), 0) % fold
    masks = [line == c for c in range(fold)]
    keep = [mask.astype(f32).astype(bf16) for mask in masks]

    half = max(1, n_sp // 2)
    upper = lax.div(sp, half)
    depth = sp + upper * (n_sp - 1 - 2 * sp)

    def mirrored(index, side):
        return index + side * (n_sp - 1 - 2 * index)

    peers = [mirrored(flip(depth, k), upper) for k in range(half)]
    quarter = max(1, half // 2)
    outer = lax.div(depth, quarter) * quarter
    inner = depth - outer
    rest = range(n_sp - half)
    peers += [mirrored(k // quarter * quarter + flip(inner, k % quarter), 1 - upper) for k in rest]
    mine = [k if k < half else half + outer + k % quarter for k in range(n_sp)]
    prepared = []

    def idle():
        for copy in stages:
            copy.wait()
        prepared.extend(prepare())

    def prepare():
        weights = shares_ref[...]
        weights = group_ref[...] * weights / jnp.sum(weights, axis=0, keepdims=True)
        table = jnp.concatenate([routes_ref[...].astype(f32), weights], axis=0)
        def look(member):
            pick = (iota((length, share), 0) == member * share + iota((length, share), 1)).astype(f32)
            return exact_dot(table, pick)

        expert = jnp.full((n_sp, share), sp, jnp.int32)
        for k in range(1, n_sp):
            expert = jnp.where(iota((n_sp, share), 0) == k, peers[k], expert)
        expert = expert.astype(f32)
        before = (iota((share, share), 0) < iota((share, share), 1)).astype(bf16)
        place = iota((per, share), 0)
        slot = jnp.where(place < 16 * main, place, 16 * main + (place - 16 * main) // fold)
        slot = slot.astype(f32)

        def choose(facts, count):
            first, second = facts[0:1] == expert, facts[1:2] == expert
            uses = jnp.where(first, 1.0, 0.0) + jnp.where(second, 1.0, 0.0)
            amounts = jnp.where(first, facts[2:3], 0.0) + jnp.where(second, facts[3:4], 0.0)
            rank = jnp.dot(uses.astype(bf16), before, preferred_element_type=f32)
            picks = [jnp.where(slot == rank[k : k + 1], uses[k : k + 1], 0.0) for k in range(count)]
            return picks, amounts

        chosen, amounts = choose(look(tp), n_sp)
        theirs = [choose(look(across(j)["tp"]), half)[0] for j in range(1, n_hi)]
        weigh = jnp.concatenate([chosen[k] * amounts[k : k + 1] for k in range(n_sp)], axis=0)
        weigh = weigh.T
        coarse = weigh.astype(bf16)
        fine = (weigh - coarse.astype(f32)).astype(bf16)
        weigh = jnp.concatenate([coarse, fine], axis=0)
        return chosen, theirs, weigh

    def across(j):
        return {"tp": flip(hi, j) * 2 + lo}

    def pack(values, extras, store):
        for i in range(main):
            store(slice(i * model, (i + 1) * model), values[16 * i : 16 * i + 16])
        folded = jnp.where(masks[0], extras[:, :piece], 0.0)
        for c in range(1, fold):
            folded = jnp.where(masks[c], extras[:, c * piece : (c + 1) * piece], folded)
        store(slice(main * model, main * model + piece), folded)

    def unpack(block):
        mains = [block[:, i * model : (i + 1) * model] for i in range(main)]
        tail = block[:, main * model :]
        return mains, jnp.concatenate([tail * keep[c] for c in range(fold)], axis=1)

    def select(picks, j):
        picks = jnp.concatenate(picks, axis=0).astype(bf16)
        rows = jnp.dot(picks, plain[j], preferred_element_type=f32)
        for k in range(picks.shape[0] // per):
            block = rows[k * per : (k + 1) * per]

            def store(columns, values):
                rows_out[j, k, :, columns] = values.astype(bf16)

            pack(block, block[16 * main :], store)

    middle = mixer_body(n_sp, n_tp, early, linked, idle, sends, mixer_in + mixer_scratch)
    middle_ref[...] = middle
    plain[0] = middle.astype(bf16)

    def crossing(j):
        return remote(plain.at[0], plain.at[j], s0.at[j], r0.at[j], across(j))

    for j in range(1, n_hi):
        go(crossing(j))
    chosen, theirs, weigh = prepared
    select(chosen, 0)

    def arrive(k):
        remote(rows_out.at[0, k], recv.at[0, k], s1.at[k], r1.at[k], {"sp": peers[k]}).wait_recv()

    def relay(k):
        arrive(k)
        for j in range(1, n_hi):
            go(remote(recv.at[0, k], recv.at[j, k], s2.at[j, k], r2.at[j, k], across(j)))

    def compute(ks):
        blocks = [(j, k) for k in ks for j in range(n_hi)]
        mains, extras = [], []
        for j, k in blocks:
            if j and k:
                remote(
                    recv.at[0, k], recv.at[j, k], s2.at[j, k], r2.at[j, k], across(j)
                ).wait_recv()
            elif k and k < half:
                arrive(k)
            a, b = unpack(recv[j, k] if k else rows_out[j, 0])
            mains += a
            extras.append(b)
        x = jnp.concatenate(mains + extras, axis=0)
        count = 16 * len(mains)

        def project(weight):
            value = jnp.concatenate(
                [jnp.dot(x, weight[i], preferred_element_type=f32) for i in range(2)], axis=1
            )
            tail = value[count:].reshape(len(blocks) * extra, fold, 2 * width)
            tail = jnp.sum(tail, axis=1, keepdims=True)
            tail = jnp.broadcast_to(tail, (len(blocks) * extra, fold, 2 * width))
            tail = tail.reshape(len(blocks) * 16, 2 * width)
            return jnp.concatenate([value[:count], tail], axis=0) if count else tail

        hidden = (jax.nn.silu(project(gate_w)) * project(linear_w)).astype(bf16)
        y = jnp.dot(hidden, down_w[...], preferred_element_type=f32)
        for i, (j, k) in enumerate(blocks):

            def store(columns, values):
                if j:
                    part[j, k, :, columns] = values.astype(bf16)
                else:
                    own[k, :, columns] = values

            pack(
                y[16 * main * i : 16 * main * (i + 1)],
                y[count + 16 * i : count + 16 * i + 16],
                store,
            )
            if j:
                go(remote(part.at[j, k], got.at[j, k], s3.at[j, k], r3.at[j, k], across(j)))

    def combine(k):
        value = own[k]
        for j in range(1, n_hi):
            remote(part.at[j, k], got.at[j, k], s3.at[j, k], r3.at[j, k], across(j)).wait_recv()
            value = value + got[j, k].astype(f32)
        if k:
            final[k] = value.astype(bf16)
            there = mine[k]
            go(remote(final.at[k], back.at[there], s4.at[k], r4.at[there], {"sp": peers[k]}))
        else:
            back[0] = value.astype(bf16)

    unit = max(1, n_sp // 8)

    def eighth(i):
        return range(i * unit, i * unit + unit)

    for i in (0, 1, 5, 7, 4, 6, 2, 3):
        for k in eighth(i):
            if k:
                there = mine[k]
                go(
                    remote(
                        rows_out.at[0, k],
                        recv.at[0, there],
                        s1.at[k],
                        r1.at[there],
                        {"sp": peers[k]},
                    )
                )
    for j in range(1, n_hi):
        crossing(j).wait_recv()
        select(theirs[j - 1], j)
        for k in range(1, half):
            go(
                remote(
                    rows_out.at[j, k], recv.at[j, k], s2.at[j, k], r2.at[j, k], {"sp": peers[k]}
                )
            )
    for fetch in fetches:
        fetch.wait()
    for copy in swaps:
        copy.wait_recv()
    for step in "r5 c0 r4 c5 c1 b0 r7 c4 b5 b1 c2 r6 c7 b4 b2 c3 c6 b7 b3 b6".split():
        ks = eighth(int(step[1:]))
        if step[0] == "c":
            compute(ks)
        else:
            for k in ks:
                (relay if step[0] == "r" else combine)(k)

    answers = []
    for k in range(n_sp):
        if k:
            remote(final.at[k], back.at[k], s4.at[k], r4.at[k], {"sp": peers[k]}).wait_recv()
        mains, tail = unpack(back[k])
        answers += mains + [tail]
    routed = jnp.dot(weigh, jnp.concatenate(answers, axis=0), preferred_element_type=f32)
    routed = routed[:share] + routed[share:]
    out_ref[...] = layer_norm(deep_alpha * middle_ref[...] + routed, gain_ref[...]).astype(bf16)
    for copy in sends:
        copy.wait_send()


def on_device(
    residual,
    mixer_input,
    log_gate,
    decay_rate,
    turn_rate,
    drive_real,
    drive_imaginary,
    read_real,
    read_imaginary,
    skip_gain,
    project_weight,
    norm_gain,
    final_gain,
    routes,
    group_weight,
    expert_weight,
    gate_weight,
    linear_weight,
    down_weight,
):
    n_sp = lax.axis_size("sp")
    n_tp = lax.axis_size("tp")
    n_hi = n_tp // 2
    length, channels = mixer_input.shape
    groups, states = decay_rate.shape[1:]
    width = groups * states
    share, model = residual.shape
    hidden = gate_weight.shape[2]
    top = routes.shape[1]
    slots = max(2, 3 * share * top // (2 * n_sp))
    main, extra, fold, piece = shape_of_block(slots, model)
    flat = lambda a: a.reshape(2, channels, states)
    staged = (mixer_input, log_gate.T, decay_rate, turn_rate)
    staged += tuple(flat(a) for a in (drive_real, drive_imaginary, read_real, read_imaginary))
    staged += (skip_gain[None, :], residual, norm_gain[None, :], project_weight)
    small = (routes.T, group_weight[None, :], expert_weight.T, final_gain[None, :])
    operands = staged + small + (gate_weight, linear_weight, down_weight)
    dma = pltpu.SemaphoreType.DMA
    block = (16, main * model + piece)
    return pl.pallas_call(
        functools.partial(layer_kernel, n_sp, n_tp, slots),
        out_shape=pltpu.VMEM((share, model), bf16),
        in_specs=[pl.BlockSpec(memory_space=pl.ANY)] * len(operands),
        out_specs=pl.BlockSpec(memory_space=pltpu.VMEM),
        scratch_shapes=[pltpu.VMEM(a.shape, a.dtype) for a in staged]
        + [
            pltpu.VMEM((4, length, width), f32),
            pltpu.VMEM((length, width), f32),
            pltpu.VMEM((8, segments, width), f32),
            pltpu.VMEM((4, segments, width), f32),
            pltpu.VMEM((8, width), f32),
            pltpu.VMEM((n_sp, 8, width), f32),
            pltpu.VMEM((length, channels), bf16),
            pltpu.VMEM((n_tp, share, channels), bf16),
            dma((len(staged),)),
            dma((n_sp,)),
            dma((n_sp,)),
            dma((n_tp,)),
            dma((n_tp,)),
        ]
        + [pltpu.VMEM(a.shape, a.dtype) for a in small]
        + [
            pltpu.VMEM((share, model), f32),
            pltpu.VMEM((n_hi, share, model), bf16),
            pltpu.VMEM((n_hi, n_sp) + block, bf16),
            pltpu.VMEM((n_hi, n_sp) + block, bf16),
            pltpu.VMEM((n_sp,) + block, f32),
            pltpu.VMEM((n_hi, n_sp) + block, bf16),
            pltpu.VMEM((n_hi, n_sp) + block, bf16),
            pltpu.VMEM((n_sp,) + block, bf16),
            pltpu.VMEM((n_sp,) + block, bf16),
            pltpu.VMEM((2, model, hidden), bf16),
            pltpu.VMEM((2, model, hidden), bf16),
            pltpu.VMEM((2 * hidden, model), bf16),
            dma((len(small),)),
            dma((3,)),
            dma((3,)),
            dma((3,)),
            dma((n_hi,)),
            dma((n_hi,)),
            dma((n_sp,)),
            dma((n_sp,)),
            dma((n_hi, n_sp)),
            dma((n_hi, n_sp)),
            dma((n_hi, n_sp)),
            dma((n_hi, n_sp)),
            dma((n_sp,)),
            dma((n_sp,)),
        ],
        compiler_params=pltpu.CompilerParams(
            collective_id=0, has_side_effects=True, vmem_limit_bytes=60 * 2**20
        ),
        name="layer",
    )(*operands)


def solution(mesh):
    placed = (
        P(("sp", "tp"), None),
        P("sp", "tp"),
        P("sp", "tp"),
        P(None, "tp", None),
        P(None, "tp", None),
        P(None, "tp", None, None),
        P(None, "tp", None, None),
        P(None, "tp", None, None),
        P(None, "tp", None, None),
        P("tp"),
        P(),
        P(),
        P(),
        P("sp", None),
        P("sp"),
        P("sp", None),
        P("sp", None, "tp"),
        P("sp", None, "tp"),
        P("sp", "tp", None),
    )
    return jax.shard_map(
        on_device, mesh=mesh, in_specs=placed, out_specs=P(("sp", "tp"), None), check_vma=False
    )
```

```python
import functools

import jax
import jax.numpy as jnp
from jax import lax
from jax.experimental import pallas as pl
from jax.experimental.pallas import tpu as pltpu
from jax.sharding import PartitionSpec as P

deep_alpha = 2.0**0.25
norm_epsilon = 1e-05
highest = lax.Precision.HIGHEST
f32 = jnp.float32
bf16 = jnp.bfloat16
segments = 8


def layer_norm(values, gain):
    center = values - jnp.mean(values, axis=-1, keepdims=True)
    spread = jnp.mean(center * center, axis=-1, keepdims=True)
    return center * lax.rsqrt(spread + norm_epsilon) * gain


def iota(shape, axis):
    return lax.broadcasted_iota(jnp.int32, shape, axis)


def exact_dot(a, b, dims=((1,), (0,))):
    return lax.dot_general(a, b, (dims, ((), ())), precision=highest, preferred_element_type=f32)


def pieces(values, count):
    out = []
    for _ in range(count):
        out.append(values.astype(bf16))
        values = values - out[-1].astype(f32)
    return out


def mixer_body(n_sp, n_tp, early, linked, idle, sends, refs):
    sources, staged = refs[:12], refs[12:24]
    (push, gate, seg, enter, total, totals, act, chan) = refs[24:32]
    (stage_sems, send_a, recv_a, send_b, recv_b) = refs[32:]
    loads = [
        pltpu.make_async_copy(source, place, stage_sems.at[i])
        for i, (source, place) in enumerate(zip(sources, staged))
    ]
    for load in loads:
        load.start()
    early()
    (x_ref, gate_ref, decay_ref, turn_ref, drive_re, drive_im) = staged[:6]
    (read_re, read_im, skip_ref, residual_ref, gain_ref, weight) = staged[6:]
    sp = lax.axis_index("sp")
    tp = lax.axis_index("tp")
    barrier = pltpu.get_barrier_semaphore()
    for k in range(1, n_sp):
        pl.semaphore_signal(barrier, inc=1, device_id={"sp": lax.rem(sp + k, n_sp)})
    for k in range(1, n_tp):
        pl.semaphore_signal(barrier, inc=1, device_id={"tp": lax.rem(tp + k, n_tp)})
    for load in loads[:6]:
        load.wait()

    length, channels = x_ref.shape
    groups, states = decay_ref.shape[1:]
    width = groups * states
    each = channels // groups
    steps = length // segments
    order = iota((length, length), 0)
    place = iota((length, length), 1)
    shuffle = (place == (order % segments) * steps + order // segments).astype(f32)
    shuffle = shuffle.astype(bf16)
    x = jnp.dot(shuffle, x_ref[...], preferred_element_type=f32)
    own = iota((groups, width), 1) // states == iota((groups, width), 0)
    diagonal = iota((channels, width), 1) // states == iota((channels, width), 0) // each

    def wide(values):
        return jnp.concatenate([values] * groups, axis=1)

    def row(values):
        return jnp.sum(jnp.where(own, wide(values), 0.0), axis=0, keepdims=True)

    def table(values):
        return jnp.where(diagonal, wide(values), 0.0)

    gates = jnp.concatenate(pieces(jnp.exp(gate_ref[...]), 3), axis=0)
    gates = lax.dot_general(shuffle, gates, (((1,), (1,)), ((), ())), preferred_element_type=f32)
    gate[...] = jnp.dot(
        gates.astype(bf16),
        jnp.concatenate([own.astype(f32).astype(bf16)] * 3, axis=0),
        preferred_element_type=f32,
    )
    twice = x.astype(bf16)
    twice = jnp.concatenate([twice, twice], axis=1)
    turn_rows = []
    for k in range(2):
        rate = decay_ref[k]
        turn = turn_ref[k]
        retain = jnp.exp(-rate)
        scale = row(jnp.sqrt(1.0 - jnp.exp(-2.0 * rate)))
        turn_rows.append((row(retain * jnp.cos(turn)), row(retain * jnp.sin(turn))))
        for i, drive in enumerate((drive_re, drive_im)):
            split = jnp.concatenate(pieces(table(drive[k]) * scale, 2), axis=0)
            push[2 * k + i] = jnp.dot(twice, split, preferred_element_type=f32)
    (f_re, f_im), (b_re, b_im) = turn_rows

    zero = jnp.zeros((segments, width), f32)
    one = jnp.ones((segments, width), f32)

    def rows_of(j):
        return pl.ds(pl.multiple_of(j * segments, segments), segments)

    def first(j, c):
        out = []
        for k, (sr, si) in enumerate(((f_re, f_im), (b_re, b_im))):
            at = rows_of(j if k == 0 else steps - 1 - j)
            kept, vr, vi = c[3 * k : 3 * k + 3]
            g = gate[at, :]
            mr, mi = g * sr, g * si
            out += [
                kept * g,
                mr * vr - mi * vi + push[2 * k, at, :],
                mr * vi + mi * vr + push[2 * k + 1, at, :],
            ]
        return tuple(out)

    def times(a, b):
        return (a[0] * b[0] - a[1] * b[1], a[0] * b[1] + a[1] * b[0])

    def power(base, count):
        if count == 1:
            return base
        root = power(base, count // 2)
        root = times(root, root)
        return times(root, base) if count % 2 else root

    ends = lax.fori_loop(0, steps, first, (one, zero, zero) * 2, unroll=4)
    for k, turned in enumerate(turn_rows):
        kept, vr, vi = ends[3 * k : 3 * k + 3]
        full = power(turned, steps)
        for i, part in enumerate((kept * full[0], kept * full[1], vr, vi)):
            seg[4 * k + i] = part

    def link(parts, c):
        ar, ai, vr, vi = parts
        return (ar * c[0] - ai * c[1] + vr, ar * c[1] + ai * c[0] + vi)

    def seg_rows(k, s):
        return [seg[4 * k + i, s : s + 1, :] for i in range(4)]

    for k in range(2):
        span = range(segments) if k == 0 else range(segments - 1, -1, -1)
        decay = (one[:1], zero[:1])
        state = (zero[:1], zero[:1])
        for s in span:
            parts = seg_rows(k, s)
            state = link(parts, state)
            decay = link(parts[:2] + [0.0, 0.0], decay)
        for i, value in enumerate(decay + state):
            total[4 * k + i : 4 * k + i + 1, :] = value
    totals[sp] = total[...]

    pl.semaphore_wait(barrier, n_sp - 1 + n_tp - 1)

    def hand(k):
        peer = lax.rem(sp + k, n_sp)
        return pltpu.make_async_remote_copy(
            src_ref=total,
            dst_ref=totals.at[sp],
            send_sem=send_a.at[k],
            recv_sem=recv_a.at[sp],
            device_id={"sp": peer},
        )

    def arrival(k):
        source = lax.rem(sp + k, n_sp)
        return pltpu.make_async_remote_copy(
            src_ref=total,
            dst_ref=totals.at[source],
            send_sem=send_a.at[k],
            recv_sem=recv_a.at[source],
            device_id={"sp": source},
        )

    for k in range(1, n_sp):
        sends.append(hand(k))
        sends[-1].start()
    for load in loads[6:9]:
        load.wait()
    tables = [value for k in range(2) for value in (table(read_re[k]), -table(read_im[k]))]
    tables = jnp.concatenate(pieces(jnp.concatenate(tables, axis=1), 2), axis=0)
    direct = skip_ref[...] * x
    for k in range(1, n_sp):
        arrival(k).wait_recv()

    linked()
    for k in range(2):
        c = (zero[:1], zero[:1])
        for d in range(n_sp) if k == 0 else range(n_sp - 1, -1, -1):
            new = link([totals[d, 4 * k + i : 4 * k + i + 1, :] for i in range(4)], c)
            counts = d < sp if k == 0 else d > sp
            c = tuple(jnp.where(counts, a, b) for a, b in zip(new, c))
        for s in range(segments) if k == 0 else range(segments - 1, -1, -1):
            enter[2 * k, s : s + 1, :] = c[0]
            enter[2 * k + 1, s : s + 1, :] = c[1]
            c = link(seg_rows(k, s), c)

    def second(j, c):
        out = []
        for k, (sr, si) in enumerate(((f_re, f_im), (b_re, b_im))):
            at = rows_of(j if k == 0 else steps - 1 - j)
            vr, vi = c[2 * k : 2 * k + 2]
            g = gate[at, :]
            mr, mi = g * sr, g * si
            new_re = mr * vr - mi * vi + push[2 * k, at, :]
            new_im = mr * vi + mi * vr + push[2 * k + 1, at, :]
            push[2 * k, at, :] = new_re
            push[2 * k + 1, at, :] = new_im
            out += [new_re, new_im]
        return tuple(out)

    lax.fori_loop(0, steps, second, tuple(enter[i] for i in range(4)), unroll=4)
    over = (((1,), (1,)), ((), ()))
    readout = direct
    for i in range(4):
        at = slice(i * width, (i + 1) * width)
        coarse, fine = pieces(push[i], 2)
        both = lax.dot_general(coarse, tables[:, at], over, preferred_element_type=f32)
        rest = lax.dot_general(fine, tables[:channels, at], over, preferred_element_type=f32)
        readout = readout + (both[:, :channels] + (both[:, channels:] + rest))
    mixed = jax.nn.gelu(readout).astype(bf16)
    act[...] = lax.dot_general(
        shuffle, mixed, (((0,), (0,)), ((), ())), preferred_element_type=f32
    ).astype(bf16)

    share = length // n_tp

    def shift(k, out):
        peer = lax.rem(tp + k, n_tp)
        return pltpu.make_async_remote_copy(
            src_ref=act.at[pl.ds(pl.multiple_of(peer * share, share), share)],
            dst_ref=chan.at[tp if out else peer],
            send_sem=send_b.at[k],
            recv_sem=recv_b.at[tp if out else peer],
            device_id={"tp": peer},
        )

    for k in range(1, n_tp):
        sends.append(shift(k, True))
        sends[-1].start()
    idle()
    chan[tp] = act[pl.ds(pl.multiple_of(tp * share, share), share), :]
    for load in loads[9:]:
        load.wait()
    for k in range(1, n_tp):
        shift(k, False).wait_recv()
    whole = jnp.concatenate([chan[m] for m in range(n_tp)], axis=1)
    branch = jnp.dot(whole, weight[...], preferred_element_type=f32)
    return layer_norm(deep_alpha * residual_ref[...].astype(f32) + branch, gain_ref[...])


def flip(base, k):
    out, bit = base, 1
    while bit <= k:
        if k & bit:
            out = out + bit - 2 * bit * lax.rem(lax.div(base, bit), 2)
        bit *= 2
    return out


def shape_of_block(slots, model):
    while slots % 16 == 0 or 16 % (slots % 16):
        slots += 1
    main, extra = slots // 16, slots % 16
    fold = 16 // extra
    return main, extra, fold, model // fold


def layer_kernel(n_sp, n_tp, slots, *refs):
    mixer_in, refs = refs[:12], refs[12:]
    small_in, refs = refs[:4], refs[4:]
    (gate_hbm, linear_hbm, down_hbm, out_ref), refs = refs[:4], refs[4:]
    mixer_scratch, refs = refs[:25], refs[25:]
    small, refs = refs[:4], refs[4:]
    (middle_ref, plain, rows_out, recv, own, part, got, final, back), refs = refs[:9], refs[9:]
    (gate_w, linear_w, down_w), refs = refs[:3], refs[3:]
    (small_sems, weight_sems, give_sems, take_sems), refs = refs[:4], refs[4:]
    s0, r0, s1, r1, s2, r2, s3, r3, s4, r4 = refs

    sp = lax.axis_index("sp")
    tp = lax.axis_index("tp")
    n_hi = n_tp // 2
    hi = lax.div(tp, 2)
    lo = lax.rem(tp, 2)
    sibling = {"tp": hi * 2 + 1 - lo}
    sends = []

    def remote(src, dst, send, receive, where):
        return pltpu.make_async_remote_copy(
            src_ref=src, dst_ref=dst, send_sem=send, recv_sem=receive, device_id=where
        )

    def go(copy):
        copy.start()
        sends.append(copy)

    width = gate_hbm.shape[2]
    homes = [(gate_hbm, gate_w.at[0]), (linear_hbm, linear_w.at[0]), (down_hbm, down_w.at[0:width])]
    others = [gate_w.at[1], linear_w.at[1], down_w.at[width : 2 * width]]
    fetches = [
        pltpu.make_async_copy(source.at[0], place, weight_sems.at[i])
        for i, (source, place) in enumerate(homes)
    ]
    swaps = [
        remote(homes[i][0].at[0], others[i], give_sems.at[i], take_sems.at[i], sibling)
        for i in range(3)
    ]
    stages = [
        pltpu.make_async_copy(source, place, small_sems.at[i])
        for i, (source, place) in enumerate(zip(small_in, small))
    ]

    def early():
        for copy in stages + fetches:
            copy.start()

    def linked():
        for copy in swaps:
            go(copy)

    routes_ref, group_ref, shares_ref, gain_ref = small

    share, model = middle_ref.shape
    length = routes_ref.shape[1]
    main, extra, fold, piece = shape_of_block(slots, model)
    per = 16 * main + 16
    line = iota((16, piece), 0) % fold
    masks = [line == c for c in range(fold)]
    keep = [mask.astype(f32).astype(bf16) for mask in masks]

    half = max(1, n_sp // 2)
    upper = lax.div(sp, half)
    depth = sp + upper * (n_sp - 1 - 2 * sp)

    def mirrored(index, side):
        return index + side * (n_sp - 1 - 2 * index)

    peers = [mirrored(flip(depth, k), upper) for k in range(half)]
    quarter = max(1, half // 2)
    outer = lax.div(depth, quarter) * quarter
    inner = depth - outer
    rest = range(n_sp - half)
    peers += [mirrored(k // quarter * quarter + flip(inner, k % quarter), 1 - upper) for k in rest]
    mine = [k if k < half else half + outer + k % quarter for k in range(n_sp)]
    prepared = []

    def idle():
        for copy in stages:
            copy.wait()
        prepared.extend(prepare())

    def prepare():
        weights = shares_ref[...]
        weights = group_ref[...] * weights / jnp.sum(weights, axis=0, keepdims=True)
        table = jnp.concatenate([routes_ref[...].astype(f32), weights], axis=0)
        def look(member):
            pick = (iota((length, share), 0) == member * share + iota((length, share), 1)).astype(f32)
            return exact_dot(table, pick)

        expert = jnp.full((n_sp, share), sp, jnp.int32)
        for k in range(1, n_sp):
            expert = jnp.where(iota((n_sp, share), 0) == k, peers[k], expert)
        expert = expert.astype(f32)
        before = (iota((share, share), 0) < iota((share, share), 1)).astype(bf16)
        place = iota((per, share), 0)
        slot = jnp.where(place < 16 * main, place, 16 * main + (place - 16 * main) // fold)
        slot = slot.astype(f32)

        def choose(facts, count):
            first, second = facts[0:1] == expert, facts[1:2] == expert
            uses = jnp.where(first, 1.0, 0.0) + jnp.where(second, 1.0, 0.0)
            amounts = jnp.where(first, facts[2:3], 0.0) + jnp.where(second, facts[3:4], 0.0)
            rank = jnp.dot(uses.astype(bf16), before, preferred_element_type=f32)
            picks = [jnp.where(slot == rank[k : k + 1], uses[k : k + 1], 0.0) for k in range(count)]
            return picks, amounts

        chosen, amounts = choose(look(tp), n_sp)
        theirs = [choose(look(across(j)["tp"]), half)[0] for j in range(1, n_hi)]
        weigh = jnp.concatenate([chosen[k] * amounts[k : k + 1] for k in range(n_sp)], axis=0)
        weigh = weigh.T
        coarse = weigh.astype(bf16)
        fine = (weigh - coarse.astype(f32)).astype(bf16)
        weigh = jnp.concatenate([coarse, fine], axis=0)
        return chosen, theirs, weigh

    def across(j):
        return {"tp": flip(hi, j) * 2 + lo}

    def pack(values, extras, store):
        for i in range(main):
            store(slice(i * model, (i + 1) * model), values[16 * i : 16 * i + 16])
        folded = jnp.where(masks[0], extras[:, :piece], 0.0)
        for c in range(1, fold):
            folded = jnp.where(masks[c], extras[:, c * piece : (c + 1) * piece], folded)
        store(slice(main * model, main * model + piece), folded)

    def unpack(block):
        mains = [block[:, i * model : (i + 1) * model] for i in range(main)]
        tail = block[:, main * model :]
        return mains, jnp.concatenate([tail * keep[c] for c in range(fold)], axis=1)

    def select(picks, j):
        picks = jnp.concatenate(picks, axis=0).astype(bf16)
        rows = jnp.dot(picks, plain[j], preferred_element_type=f32)
        for k in range(picks.shape[0] // per):
            block = rows[k * per : (k + 1) * per]

            def store(columns, values):
                rows_out[j, k, :, columns] = values.astype(bf16)

            pack(block, block[16 * main :], store)

    middle = mixer_body(n_sp, n_tp, early, linked, idle, sends, mixer_in + mixer_scratch)
    middle_ref[...] = middle
    plain[0] = middle.astype(bf16)

    def crossing(j):
        return remote(plain.at[0], plain.at[j], s0.at[j], r0.at[j], across(j))

    for j in range(1, n_hi):
        go(crossing(j))
    chosen, theirs, weigh = prepared
    select(chosen, 0)

    def arrive(k):
        remote(rows_out.at[0, k], recv.at[0, k], s1.at[k], r1.at[k], {"sp": peers[k]}).wait_recv()

    def relay(k):
        arrive(k)
        for j in range(1, n_hi):
            go(remote(recv.at[0, k], recv.at[j, k], s2.at[j, k], r2.at[j, k], across(j)))

    def compute(ks):
        blocks = [(j, k) for k in ks for j in range(n_hi)]
        mains, extras = [], []
        for j, k in blocks:
            if j and k:
                remote(
                    recv.at[0, k], recv.at[j, k], s2.at[j, k], r2.at[j, k], across(j)
                ).wait_recv()
            elif k and k < half:
                arrive(k)
            a, b = unpack(recv[j, k] if k else rows_out[j, 0])
            mains += a
            extras.append(b)
        x = jnp.concatenate(mains + extras, axis=0)
        count = 16 * len(mains)

        def project(weight):
            value = jnp.concatenate(
                [jnp.dot(x, weight[i], preferred_element_type=f32) for i in range(2)], axis=1
            )
            tail = value[count:].reshape(len(blocks) * extra, fold, 2 * width)
            tail = jnp.sum(tail, axis=1, keepdims=True)
            tail = jnp.broadcast_to(tail, (len(blocks) * extra, fold, 2 * width))
            tail = tail.reshape(len(blocks) * 16, 2 * width)
            return jnp.concatenate([value[:count], tail], axis=0) if count else tail

        hidden = (jax.nn.silu(project(gate_w)) * project(linear_w)).astype(bf16)
        y = jnp.dot(hidden, down_w[...], preferred_element_type=f32)
        for i, (j, k) in enumerate(blocks):

            def store(columns, values):
                if j:
                    part[j, k, :, columns] = values.astype(bf16)
                else:
                    own[k, :, columns] = values

            pack(
                y[16 * main * i : 16 * main * (i + 1)],
                y[count + 16 * i : count + 16 * i + 16],
                store,
            )
            if j:
                go(remote(part.at[j, k], got.at[j, k], s3.at[j, k], r3.at[j, k], across(j)))

    def combine(k):
        value = own[k]
        for j in range(1, n_hi):
            remote(part.at[j, k], got.at[j, k], s3.at[j, k], r3.at[j, k], across(j)).wait_recv()
            value = value + got[j, k].astype(f32)
        if k:
            final[k] = value.astype(bf16)
            there = mine[k]
            go(remote(final.at[k], back.at[there], s4.at[k], r4.at[there], {"sp": peers[k]}))
        else:
            back[0] = value.astype(bf16)

    unit = max(1, n_sp // 8)

    def eighth(i):
        return range(i * unit, i * unit + unit)

    for i in (0, 1, 5, 7, 4, 6, 2, 3):
        for k in eighth(i):
            if k:
                there = mine[k]
                go(
                    remote(
                        rows_out.at[0, k],
                        recv.at[0, there],
                        s1.at[k],
                        r1.at[there],
                        {"sp": peers[k]},
                    )
                )
    for j in range(1, n_hi):
        crossing(j).wait_recv()
        select(theirs[j - 1], j)
        for k in range(1, half):
            go(
                remote(
                    rows_out.at[j, k], recv.at[j, k], s2.at[j, k], r2.at[j, k], {"sp": peers[k]}
                )
            )
    for fetch in fetches:
        fetch.wait()
    for copy in swaps:
        copy.wait_recv()
    for step in "r5 c0 r4 c5 c1 b0 r7 c4 b5 c2 b1 r6 c7 b4 c3 b2 c6 b7 b3 b6".split():
        ks = eighth(int(step[1:]))
        if step[0] == "c":
            compute(ks)
        else:
            for k in ks:
                (relay if step[0] == "r" else combine)(k)

    answers = []
    for k in range(n_sp):
        if k:
            remote(final.at[k], back.at[k], s4.at[k], r4.at[k], {"sp": peers[k]}).wait_recv()
        mains, tail = unpack(back[k])
        answers += mains + [tail]
    routed = jnp.dot(weigh, jnp.concatenate(answers, axis=0), preferred_element_type=f32)
    routed = routed[:share] + routed[share:]
    out_ref[...] = layer_norm(deep_alpha * middle_ref[...] + routed, gain_ref[...]).astype(bf16)
    for copy in sends:
        copy.wait_send()


def on_device(
    residual,
    mixer_input,
    log_gate,
    decay_rate,
    turn_rate,
    drive_real,
    drive_imaginary,
    read_real,
    read_imaginary,
    skip_gain,
    project_weight,
    norm_gain,
    final_gain,
    routes,
    group_weight,
    expert_weight,
    gate_weight,
    linear_weight,
    down_weight,
):
    n_sp = lax.axis_size("sp")
    n_tp = lax.axis_size("tp")
    n_hi = n_tp // 2
    length, channels = mixer_input.shape
    groups, states = decay_rate.shape[1:]
    width = groups * states
    share, model = residual.shape
    hidden = gate_weight.shape[2]
    top = routes.shape[1]
    slots = max(2, 3 * share * top // (2 * n_sp))
    main, extra, fold, piece = shape_of_block(slots, model)
    flat = lambda a: a.reshape(2, channels, states)
    staged = (mixer_input, log_gate.T, decay_rate, turn_rate)
    staged += tuple(flat(a) for a in (drive_real, drive_imaginary, read_real, read_imaginary))
    staged += (skip_gain[None, :], residual, norm_gain[None, :], project_weight)
    small = (routes.T, group_weight[None, :], expert_weight.T, final_gain[None, :])
    operands = staged + small + (gate_weight, linear_weight, down_weight)
    dma = pltpu.SemaphoreType.DMA
    block = (16, main * model + piece)
    return pl.pallas_call(
        functools.partial(layer_kernel, n_sp, n_tp, slots),
        out_shape=pltpu.VMEM((share, model), bf16),
        in_specs=[pl.BlockSpec(memory_space=pl.ANY)] * len(operands),
        out_specs=pl.BlockSpec(memory_space=pltpu.VMEM),
        scratch_shapes=[pltpu.VMEM(a.shape, a.dtype) for a in staged]
        + [
            pltpu.VMEM((4, length, width), f32),
            pltpu.VMEM((length, width), f32),
            pltpu.VMEM((8, segments, width), f32),
            pltpu.VMEM((4, segments, width), f32),
            pltpu.VMEM((8, width), f32),
            pltpu.VMEM((n_sp, 8, width), f32),
            pltpu.VMEM((length, channels), bf16),
            pltpu.VMEM((n_tp, share, channels), bf16),
            dma((len(staged),)),
            dma((n_sp,)),
            dma((n_sp,)),
            dma((n_tp,)),
            dma((n_tp,)),
        ]
        + [pltpu.VMEM(a.shape, a.dtype) for a in small]
        + [
            pltpu.VMEM((share, model), f32),
            pltpu.VMEM((n_hi, share, model), bf16),
            pltpu.VMEM((n_hi, n_sp) + block, bf16),
            pltpu.VMEM((n_hi, n_sp) + block, bf16),
            pltpu.VMEM((n_sp,) + block, f32),
            pltpu.VMEM((n_hi, n_sp) + block, bf16),
            pltpu.VMEM((n_hi, n_sp) + block, bf16),
            pltpu.VMEM((n_sp,) + block, bf16),
            pltpu.VMEM((n_sp,) + block, bf16),
            pltpu.VMEM((2, model, hidden), bf16),
            pltpu.VMEM((2, model, hidden), bf16),
            pltpu.VMEM((2 * hidden, model), bf16),
            dma((len(small),)),
            dma((3,)),
            dma((3,)),
            dma((3,)),
            dma((n_hi,)),
            dma((n_hi,)),
            dma((n_sp,)),
            dma((n_sp,)),
            dma((n_hi, n_sp)),
            dma((n_hi, n_sp)),
            dma((n_hi, n_sp)),
            dma((n_hi, n_sp)),
            dma((n_sp,)),
            dma((n_sp,)),
        ],
        compiler_params=pltpu.CompilerParams(
            collective_id=0, has_side_effects=True, vmem_limit_bytes=60 * 2**20
        ),
        name="layer",
    )(*operands)


def solution(mesh):
    placed = (
        P(("sp", "tp"), None),
        P("sp", "tp"),
        P("sp", "tp"),
        P(None, "tp", None),
        P(None, "tp", None),
        P(None, "tp", None, None),
        P(None, "tp", None, None),
        P(None, "tp", None, None),
        P(None, "tp", None, None),
        P("tp"),
        P(),
        P(),
        P(),
        P("sp", None),
        P("sp"),
        P("sp", None),
        P("sp", None, "tp"),
        P("sp", None, "tp"),
        P("sp", "tp", None),
    )
    return jax.shard_map(
        on_device, mesh=mesh, in_specs=placed, out_specs=P(("sp", "tp"), None), check_vma=False
    )
```
